32 devices in a mesh: sp: 8 (over z, core), tp: 4 (over y, x).
Axes of the slice: x: 2, y: 2, z: 4, core: 2. Of those that a mesh axis runs over, the one named last changes fastest.
Arguments:
- stream: bfloat16 [3072, 2048], P('sp', 'tp'), may hold values from -6 to 6
- doc_ids: int32 [3072], P('sp'), may hold values from 0 to 1, never falling along the last dimension, each value on 1 to 2304 neighbouring positions
- w_value: bfloat16 [3, 2048, 2048], P(None, None, 'tp'), may hold values from -0.125 to 0.125
- w_gate: bfloat16 [3, 2048, 2048], P(None, None, 'tp'), may hold values from -0.125 to 0.125
- conv_kernel: bfloat16 [3, 31, 2048], P(None, None, 'tp'), may hold values from -4 to 4
- conv_gain: float32 [3, 2048], replicated, may hold values from 0.1 to 1.9
- conv_shift: float32 [3, 2048], replicated, may hold values from -3 to 3
- w_proj: bfloat16 [3, 2048, 2048], P(None, None, 'tp'), may hold values from -0.125 to 0.125
- out_gain: float32 [3, 2048], replicated, may hold values from 0.1 to 1.9
- out_shift: float32 [3, 2048], replicated, may hold values from -3 to 3
Outputs:
- result: bfloat16 [3072, 2048], P('sp', 'tp')
The draws below stay inside these ranges and needn't reach their ends.
All inputs are finite; a program needn't handle non-finite values.
Results may differ from the reference program's by a relative error of at most 0.013.
Values may be sent and summed in bfloat16 or wider, within the bound.
A program may use at most 64 MiB of HBM per device.

```python
import math
import jax
import jax.numpy as jnp
import numpy as np
from jax import lax

D = 2048
DC = 2048
KERNEL = 31
LAYERS = 3
TOK_DEV = 384
HALF = 15
TOKENS = 3072


def draw_conv_kernel(key, part):
    first = jax.random.fold_in(key, 11)
    second = jax.random.fold_in(key, 12)
    rough = jax.random.uniform(second, (DC,), jnp.float32, 0.5, 1.5)
    base = jnp.clip(jax.random.normal(first, (LAYERS, KERNEL, DC), jnp.float32), -4.0, 4.0)
    ramp = jnp.exp(jnp.linspace(math.log(0.4), math.log(2.0), DC))
    return (base * (ramp * rough)[None, None, :] * KERNEL ** (-0.5)).astype(jnp.bfloat16)


def steps_of(rng, shape, pieces, smallest, largest):
    def one(axis_at, shards_of):
        steps = jax.random.uniform(jax.random.fold_in(jax.random.fold_in(rng, 6), axis_at), (shards_of,), jnp.float32, smallest / len(pieces), largest / len(pieces))
        return jnp.repeat(jnp.exp(steps), shape[axis_at] // shards_of).reshape((-1,) + (1,) * (len(shape) - axis_at - 1))

    level = one(*pieces[0])
    for cut in pieces[1:]:
        level = level * one(*cut)
    return level


def split_up(count, total, reach, slope):
    loads = [(1 << 20) // math.isqrt(grade ** slope) + 1 for grade in range(2, count + 1)]
    surplus, counts = total - reach - (count - 1), [1] * (count - 1)
    while surplus > 0:
        free = [i for i in range(count - 1) if counts[i] < reach]
        pool, left = sum([loads[i] for i in free]), surplus
        for i in free:
            more = min(reach - counts[i], max(1, left * loads[i] // pool), surplus)
            counts[i] = counts[i] + more
            surplus = surplus - more
    return np.array([reach] + counts)


def ragged(key, amount, total, limit, lean):
    if amount == 2:
        one = jax.random.randint(key, (), max(1, total - limit), min(limit, total - 1) + 1)
        return jnp.stack([one, total - one])
    lengths = jnp.asarray(split_up(amount, total, limit, lean), jnp.int32)
    twos = (amount - 1) // 2
    donor, sink = lengths[1:1 + 2 * twos:2], lengths[2:2 + 2 * twos:2]
    slack = jnp.minimum(donor - 1, limit - sink)
    passed = jax.random.randint(jax.random.fold_in(key, 1), (twos,), 0, 1 << 20) % (slack + 1)
    lengths = lengths.at[1:1 + 2 * twos:2].set(donor - passed).at[2:2 + 2 * twos:2].set(sink + passed)
    return lengths[jax.random.permutation(jax.random.fold_in(key, 2), amount)]


def bell_draw(own_key, extent, scale, limit, shards=(), held_as=jnp.bfloat16):
    level = steps_of(own_key, extent, shards, -0.22, 0.18) if shards else 1.0
    drawn = jax.random.normal(own_key, extent, jnp.float32) * scale * level
    return jnp.minimum(jnp.maximum(drawn, -limit), limit).astype(held_as)


def setup_inputs(seed: int = 0) -> dict:
    arg_keys = jax.random.split(jax.random.key(seed), 11)
    stream = bell_draw(arg_keys[0], (TOKENS, D), 1.0, 6.0, ((0, 8), (1, 4)))
    doc_ids = jnp.searchsorted(jnp.cumsum(ragged(arg_keys[1], TOKENS // (3 * TOK_DEV), TOKENS, 6 * TOK_DEV, 2)), jnp.arange(TOKENS), side="right").astype(jnp.int32)
    w_value = bell_draw(arg_keys[2], (LAYERS, D, DC), D ** -0.5, 0.125, ((2, 4),))
    w_gate = bell_draw(arg_keys[3], (LAYERS, D, DC), D ** -0.5, 0.125, ((2, 4),))
    conv_kernel = draw_conv_kernel(jax.random.fold_in(arg_keys[10], 71), 0)
    conv_gain = jnp.clip(1.0 + 0.18 * jax.random.normal(arg_keys[5], (LAYERS, DC), jnp.float32), 0.1, 1.9)
    conv_shift = bell_draw(arg_keys[6], (LAYERS, DC), 0.5, 3.0, (), jnp.float32)
    w_proj = bell_draw(arg_keys[7], (LAYERS, DC, D), DC ** -0.5, 0.125, ((2, 4),))
    out_gain = jnp.clip(1.0 + 0.18 * jax.random.normal(arg_keys[8], (LAYERS, D), jnp.float32), 0.1, 1.9)
    out_shift = bell_draw(arg_keys[9], (LAYERS, D), 0.5, 3.0, (), jnp.float32)
    return dict(stream=stream, doc_ids=doc_ids, w_value=w_value, w_gate=w_gate, conv_kernel=conv_kernel, conv_gain=conv_gain, conv_shift=conv_shift, w_proj=w_proj, out_gain=out_gain, out_shift=out_shift)


ALPHA = 2.0 ** 0.25
EPS = 1e-05

def reference(stream, doc_ids, w_value, w_gate, conv_kernel, conv_gain, conv_shift, w_proj, out_gain, out_shift):
    hidden = stream
    seg_pad = jnp.pad(doc_ids, (HALF, HALF), constant_values=-1)
    for layer in range(LAYERS):
        lin = jnp.dot(hidden, w_value[layer], preferred_element_type=jnp.float32)
        gat = jnp.dot(hidden, w_gate[layer], preferred_element_type=jnp.float32)
        glu = (lin * jax.nn.sigmoid(gat)).astype(jnp.bfloat16)
        padded = jnp.pad(glu.astype(jnp.float32), ((HALF, HALF), (0, 0)))
        taps = conv_kernel[layer].astype(jnp.float32)
        total = jnp.zeros((TOKENS, DC), jnp.float32)
        for k in range(KERNEL):
            keep = (seg_pad[k:k + TOKENS] == doc_ids).astype(jnp.float32)[:, None]
            total = total + padded[k:k + TOKENS] * keep * taps[k][None, :]
        conv = total.astype(jnp.bfloat16).astype(jnp.float32)
        centre = lax.optimization_barrier(jnp.mean(conv, axis=1, keepdims=True))
        spread = lax.optimization_barrier(jnp.mean(jnp.square(conv - centre), axis=1, keepdims=True))
        normed = (conv - centre) * jax.lax.rsqrt(spread + EPS) * conv_gain[layer] + conv_shift[layer]
        act = jax.nn.silu(normed).astype(jnp.bfloat16)
        mixed = ALPHA * hidden.astype(jnp.float32) + jnp.dot(act, w_proj[layer], preferred_element_type=jnp.float32)
        mean_z = lax.optimization_barrier(jnp.mean(mixed, axis=1, keepdims=True))
        var_z = lax.optimization_barrier(jnp.mean(jnp.square(mixed - mean_z), axis=1, keepdims=True))
        hidden = ((mixed - mean_z) * jax.lax.rsqrt(var_z + EPS) * out_gain[layer] + out_shift[layer]).astype(jnp.bfloat16)
    return hidden
```

```python
import functools

import jax
import jax.numpy as jnp
from jax import lax
from jax.experimental import pallas as pl
from jax.experimental.pallas import tpu as pltpu
from jax.sharding import PartitionSpec as P

KERNEL = 31
HALF = 15
PAD = 16
CHUNK = 96
LANES = 128
ROW_BLOCK = 16
CONV_BLOCK = 32
SUM_BLOCK = 32
ALPHA = 2.0**0.25
EPS = 1e-05
MESH = pl.DeviceIdType.MESH


FIRST = (
    ("send", 0),
    ("send", 1),
    ("hr0", 0),
    ("hr1", 0),
    ("send", 2),
    ("hr0", 1),
    ("hr1", 1),
    ("send", 3),
    ("docs", 0),
    ("hr1", 2),
)
REPEAT = (
    ("glu", 0, 0),
    ("hr0", 2, 0),
    ("glu", 1, 0),
    ("hr1", 3, 0),
    ("hr0", 3, 0),
    ("conv", 0, 0),
    ("glu", 2, 0),
    ("conv", 1, 0),
    ("glu", 3, 0),
    ("cr1", 0, 0),
    ("cr0", 0, 0),
    ("conv", 2, 0),
    ("cr0", 1, 0),
    ("cr1", 1, 0),
    ("conv", 3, 0),
    ("cr1", 2, 0),
    ("cr0", 2, 0),
    ("proj", 0, 0),
    ("cr0", 3, 0),
    ("cr1", 3, 0),
    ("proj", 1, 0),
    ("hr1", 0, 1),
    ("proj", 2, 0),
    ("hr0", 0, 1),
    ("hr1", 1, 1),
    ("hr0", 1, 1),
    ("hr1", 2, 1),
    ("proj", 3, 0),
)


def plan(chunks):
    if chunks == 4:
        return FIRST, REPEAT
    first = [("send", p) for p in range(chunks)] + [("docs", 0)]
    repeat = [("hr%d" % i, p, 0) for p in range(chunks) for i in range(2)]
    repeat += [("glu", p, 0) for p in range(chunks)]
    repeat += [("conv", p, 0) for p in range(chunks)]
    repeat += [("cr%d" % i, p, 0) for p in range(chunks) for i in range(2)]
    repeat += [("proj", p, 0) for p in range(chunks)]
    return first, repeat


def sigmoid(v):
    return 0.5 * jnp.tanh(0.5 * v) + 0.5


def silu(v):
    return v * sigmoid(v)


def kernel(
    n,
    n_sp,
    first,
    repeat,
    stream,
    docs,
    wv_hbm,
    wg_hbm,
    taps_in,
    conv_gain_in,
    conv_shift_in,
    wp_hbm,
    out_gain_in,
    out_shift_in,
    out,
    conv_gain,
    conv_shift,
    out_gain,
    out_shift,
    wv,
    wg,
    wp,
    hbuf,
    cbuf,
    hn,
    act,
    glu,
    docpad,
    taps,
    zf,
    st_send,
    st_recv,
    means,
    scales,
    w_sem,
    s_sem,
    r_sem,
    hs_sem,
    hr_sem,
    ds_sem,
    dr_sem,
    ss_sem,
    sr_sem,
):
    rows, local_d = stream.shape
    layers, width, local_c = wv.shape
    groups = local_c // LANES
    chunks = rows // CHUNK
    half = CHUNK // 2
    relayed = n == 4
    me = lax.axis_index("tp")
    sp = lax.axis_index("sp")
    parity = lax.rem(sp, 2)

    for layer in range(layers):
        for i, (src, dst) in enumerate(((wv_hbm, wv), (wg_hbm, wg), (wp_hbm, wp))):
            pltpu.make_async_copy(src.at[layer], dst.at[layer], w_sem.at[i, layer]).start()

    def wait_weight(i, layer):
        src, dst = ((wv_hbm, wv), (wg_hbm, wg), (wp_hbm, wp))[i]
        pltpu.make_async_copy(src.at[layer], dst.at[layer], w_sem.at[i, layer]).wait()

    barrier = pltpu.get_barrier_semaphore()
    for j in range(1, n):
        pl.semaphore_signal(
            barrier, inc=1, device_id={"tp": lax.rem(me + j, n)}, device_id_type=MESH
        )

    @pl.when(sp > 0)
    def _():
        pl.semaphore_signal(barrier, inc=1, device_id={"sp": sp - 1}, device_id_type=MESH)

    @pl.when(sp < n_sp - 1)
    def _():
        pl.semaphore_signal(barrier, inc=1, device_id={"sp": sp + 1}, device_id_type=MESH)

    docpad[pl.ds(PAD, rows), :] = docs[...]
    taps[:, pl.ds(0, KERNEL), :] = taps_in[...].astype(jnp.float32)
    hbuf[0, me] = stream[...]
    for layer in range(layers):
        conv_gain[layer] = conv_gain_in[pl.ds(layer, 1), :]
        conv_shift[layer] = conv_shift_in[pl.ds(layer, 1), :]
        out_gain[layer] = out_gain_in[pl.ds(layer, 1), :]
        out_shift[layer] = out_shift_in[pl.ds(layer, 1), :]
    st_send[...] = jnp.zeros((chunks, 8, LANES), jnp.float32)
    st_recv[...] = jnp.zeros((chunks, LANES, LANES), jnp.float32)

    @pl.when(sp == 0)
    def _():
        docpad[pl.ds(0, PAD), :] = jnp.full((PAD, LANES), -1, jnp.int32)
        glu[:, :, pl.ds(0, PAD), :] = jnp.zeros((layers, groups, PAD, LANES), jnp.float32)

    @pl.when(sp == n_sp - 1)
    def _():
        docpad[pl.ds(PAD + rows, PAD), :] = jnp.full((PAD, LANES), -1, jnp.int32)
        glu[:, :, pl.ds(PAD + rows, PAD), :] = jnp.zeros(
            (layers, groups, PAD, LANES), jnp.float32
        )

    beside = (sp > 0).astype(jnp.int32) + (sp < n_sp - 1).astype(jnp.int32)
    pl.semaphore_wait(barrier, n - 1 + beside)

    def first_row(p):
        return pl.multiple_of((p + parity * (chunks - 1 - 2 * p)) * CHUNK, CHUNK)

    starts = [first_row(p) for p in range(chunks)]

    if relayed:
        near_x = me + 1 - 2 * lax.rem(me, 2)
        near_y = me + 2 - 4 * (me // 2)

    def own_copies(buf, layer, kind, p, source=None):
        a = 2 * layer + kind
        if relayed:
            plan = [(near_x, 0, 0), (near_y, half, 1), (near_x, half, 4), (near_y, 0, 5)]
            size = half
        else:
            plan = [(lax.rem(me + j, n), 0, j - 1) for j in range(1, n)]
            size = CHUNK
        copies = []
        for peer, offset, i in plan:
            part = pl.ds(pl.multiple_of(starts[p] + offset, half), size)
            block = buf.at[layer, me, part, :]
            copies.append(
                pltpu.make_async_remote_copy(
                    src_ref=block if source is None else source.at[part, :],
                    dst_ref=block,
                    send_sem=s_sem.at[a, p, i],
                    recv_sem=r_sem.at[a, p, i],
                    device_id={"tp": peer},
                    device_id_type=MESH,
                )
            )
        return copies

    def relay_copies(buf, layer, kind, p):
        a = 2 * layer + kind
        out_copies = []
        for i, (origin, target) in enumerate(((near_x, near_y), (near_y, near_x))):
            part = buf.at[
                layer, origin, pl.ds(pl.multiple_of(starts[p] + i * half, half), half), :
            ]
            out_copies.append(
                pltpu.make_async_remote_copy(
                    src_ref=part,
                    dst_ref=part,
                    send_sem=s_sem.at[a, p, 2 + i],
                    recv_sem=r_sem.at[a, p, 2 + i],
                    device_id={"tp": target},
                    device_id_type=MESH,
                )
            )
        return out_copies

    def send(buf, layer, kind, p, source=None):
        for copy in own_copies(buf, layer, kind, p, source):
            copy.start()

    def relay(buf, layer, kind, p, i):
        if relayed:
            own_copies(buf, layer, kind, p)[i].wait_recv()
            relay_copies(buf, layer, kind, p)[i].start()

    def finish(buf, layer, kind, p):
        if relayed:
            for copy in own_copies(buf, layer, kind, p)[2:] + relay_copies(buf, layer, kind, p):
                copy.wait_recv()
        else:
            for copy in own_copies(buf, layer, kind, p):
                copy.wait_recv()

    def drain(buf, layer, kind, p):
        for copy in own_copies(buf, layer, kind, p):
            copy.wait_send()
        if relayed:
            for copy in relay_copies(buf, layer, kind, p):
                copy.wait_send()

    def edge(e):
        side = lax.rem(parity + e, 2)
        partner = sp - 1 + 2 * side
        there = (partner >= 0) & (partner < n_sp)
        src = pl.multiple_of(PAD + side * (rows - PAD), PAD)
        dst = pl.multiple_of((1 - side) * (PAD + rows), PAD)
        return partner, there, src, dst

    def halo_copy(layer, e):
        partner, there, src, dst = edge(e)
        return there, pltpu.make_async_remote_copy(
            src_ref=glu.at[layer, :, pl.ds(src, PAD), :],
            dst_ref=glu.at[layer, :, pl.ds(dst, PAD), :],
            send_sem=hs_sem.at[layer, e],
            recv_sem=hr_sem.at[layer, e],
            device_id={"sp": partner},
            device_id_type=MESH,
        )

    def doc_copy(e):
        partner, there, src, dst = edge(e)
        return there, pltpu.make_async_remote_copy(
            src_ref=docs.at[pl.ds(pl.multiple_of(src - PAD, PAD), PAD), :],
            dst_ref=docpad.at[pl.ds(dst, PAD), :],
            send_sem=ds_sem.at[e],
            recv_sem=dr_sem.at[e],
            device_id={"sp": partner},
            device_id_type=MESH,
        )

    def on(pair, what):
        there, copy = pair

        @pl.when(there)
        def _():
            getattr(copy, what)()

    def normalize(load, store, gain, shift, piece, finish_with):
        lanes = range(piece // LANES)

        count = width // LANES

        def measure(i, carry):
            at = pl.multiple_of(i * SUM_BLOCK, SUM_BLOCK)
            pivot = None
            for s in range(n):
                part = load(s, at, SUM_BLOCK)
                for g in lanes:
                    value = part[:, g * LANES : (g + 1) * LANES].astype(jnp.float32)
                    if pivot is None:
                        pivot = value
                        first = jnp.zeros_like(value)
                        second = jnp.zeros_like(value)
                    else:
                        off = value - pivot
                        first = first + off
                        second = second + off * off
            middle = first * (1.0 / count)
            means[pl.ds(at, SUM_BLOCK), :] = pivot + middle
            scales[pl.ds(at, SUM_BLOCK), :] = jnp.maximum(second - first * middle, 0.0)
            return carry

        lax.fori_loop(0, CHUNK // SUM_BLOCK, measure, 0, unroll=True)
        middle = means[...]
        mean = jnp.sum(middle, axis=1, keepdims=True) * (1.0 / LANES)
        off = middle - mean
        spread = jnp.sum(scales[...] + off * off * count, axis=1, keepdims=True)
        means[...] = jnp.broadcast_to(mean, (CHUNK, LANES))
        scales[...] = jnp.broadcast_to(lax.rsqrt(spread * (1.0 / width) + EPS), (CHUNK, LANES))

        def body(i, carry):
            at = pl.multiple_of(i * ROW_BLOCK, ROW_BLOCK)
            mean = means[pl.ds(at, ROW_BLOCK), :]
            scale = scales[pl.ds(at, ROW_BLOCK), :]
            for s in range(n):
                part = load(s, at, ROW_BLOCK)
                for g in lanes:
                    value = part[:, g * LANES : (g + 1) * LANES].astype(jnp.float32)
                    column = s * piece + g * LANES
                    value = (value - mean) * scale * gain(column) + shift(column)
                    store(s, at, g * LANES, finish_with(value).astype(jnp.bfloat16))
            return carry

        lax.fori_loop(0, CHUNK // ROW_BLOCK, body, 0, unroll=2)

    def make_glu(layer, p):
        r0 = starts[p]
        span = pl.ds(r0, CHUNK)

        @pl.when(layer == 0)
        def _():
            for s in range(n):
                hn[span, pl.ds(s * local_d, local_d)] = hbuf[0, s, span, :]

        @pl.when(layer > 0)
        def _():
            before = jnp.maximum(layer - 1, 0)
            normalize(
                lambda s, at, count: hbuf[layer, s, pl.ds(r0 + at, count), :],
                lambda s, at, c, v: hn.__setitem__(
                    (pl.ds(r0 + at, ROW_BLOCK), pl.ds(s * local_d + c, LANES)), v
                ),
                lambda c: out_gain[before, :, pl.ds(c, LANES)],
                lambda c: out_shift[before, :, pl.ds(c, LANES)],
                local_d,
                lambda v: v,
            )

        x = hn[span, :]
        lin = jnp.dot(x, wv[layer], preferred_element_type=jnp.float32)
        gat = jnp.dot(x, wg[layer], preferred_element_type=jnp.float32)
        gated = (lin * sigmoid(gat)).astype(jnp.bfloat16).astype(jnp.float32)
        at = pl.multiple_of(r0 + PAD, PAD)
        for g in range(groups):
            glu[layer, g, pl.ds(at, CHUNK), :] = gated[:, g * LANES : (g + 1) * LANES]

    def convolve(layer, p):
        r0 = starts[p]

        def body(i, carry):
            t0 = pl.multiple_of(r0 + i * CONV_BLOCK, CONV_BLOCK)
            centre = docpad[pl.ds(t0 + PAD, CONV_BLOCK), :]
            totals = [jnp.zeros((CONV_BLOCK, LANES), jnp.float32) for _ in range(groups)]
            for k in range(KERNEL):
                at = pl.ds(t0 + k + PAD - HALF, CONV_BLOCK)
                keep = docpad[at, :] == centre
                for g in range(groups):
                    tap = taps[layer, pl.ds(k, 1), pl.ds(g * LANES, LANES)]
                    totals[g] = totals[g] + jnp.where(keep, glu[layer, g, at, :], 0.0) * tap
            for g in range(groups):
                cbuf[layer, me, pl.ds(t0, CONV_BLOCK), pl.ds(g * LANES, LANES)] = totals[
                    g
                ].astype(jnp.bfloat16)
            return carry

        lax.fori_loop(0, CHUNK // CONV_BLOCK, body, 0)

    def project(layer, p):
        r0 = starts[p]
        span = pl.ds(r0, CHUNK)
        normalize(
            lambda s, at, count: cbuf[layer, s, pl.ds(r0 + at, count), :],
            lambda s, at, c, v: act.__setitem__(
                (pl.ds(at, ROW_BLOCK), pl.ds(s * local_c + c, LANES)), v
            ),
            lambda c: conv_gain[layer, :, pl.ds(c, LANES)],
            lambda c: conv_shift[layer, :, pl.ds(c, LANES)],
            local_c,
            silu,
        )
        z = jnp.dot(act[...], wp[layer], preferred_element_type=jnp.float32)
        own = hn[span, pl.ds(pl.multiple_of(me * local_d, LANES), local_d)]
        z = z + ALPHA * own.astype(jnp.float32)

        @pl.when(layer < layers - 1)
        def _():
            after = jnp.minimum(layer + 1, layers - 1)
            hbuf[after, me, span, :] = z.astype(jnp.bfloat16)
            send(hbuf, after, 0, p)

        @pl.when(layer == layers - 1)
        def _():
            zf[span, :] = z
            total = jnp.sum(z, axis=1, keepdims=True)
            off = z - total * (1.0 / local_d)
            spread = jnp.sum(off * off, axis=1, keepdims=True)
            lane = lax.broadcasted_iota(jnp.int32, (CHUNK, LANES), 1)
            tile = jnp.where(lane == 0, total, jnp.where(lane == 1, spread, 0.0))
            stats = jnp.transpose(tile)[:8, :]
            st_send[p, :, pl.ds(0, CHUNK)] = stats
            st_recv[p, pl.ds(pl.multiple_of(me * 8, 8), 8), pl.ds(0, CHUNK)] = stats
            for copy in stat_copies(p):
                copy.start()

    def stat_copies(p):
        return [
            pltpu.make_async_remote_copy(
                src_ref=st_send.at[p],
                dst_ref=st_recv.at[p, pl.ds(pl.multiple_of(me * 8, 8), 8), :],
                send_sem=ss_sem.at[p, j - 1],
                recv_sem=sr_sem.at[p, j - 1],
                device_id={"tp": lax.rem(me + j, n)},
                device_id_type=MESH,
            )
            for j in range(1, n)
        ]

    def step(what, p, layer):
        if what == "send":
            send(hbuf, 0, 0, p, source=stream)
        elif what in ("hr0", "hr1"):
            relay(hbuf, layer, 0, p, int(what[2]))
        elif what in ("cr0", "cr1"):
            relay(cbuf, layer, 1, p, int(what[2]))
        elif what == "glu":
            finish(hbuf, layer, 0, p)
            if p == 0:
                wait_weight(0, layer)
                wait_weight(1, layer)
            make_glu(layer, p)
            if p == 0:
                on(halo_copy(layer, 0), "start")
            if p == chunks - 1:
                on(halo_copy(layer, 1), "start")
        elif what == "conv":
            if p == 0:
                on(halo_copy(layer, 0), "wait_recv")
            if p == chunks - 1:
                on(halo_copy(layer, 1), "wait_recv")
            convolve(layer, p)
            send(cbuf, layer, 1, p)
        elif what == "proj":
            if p == 0:
                wait_weight(2, layer)
            finish(cbuf, layer, 1, p)
            project(layer, p)

    for what, p in first:
        if what == "docs":
            for e in range(2):
                on(doc_copy(e), "start")
            for e in range(2):
                on(doc_copy(e), "wait")
        else:
            step(what, p, 0)

    def one_layer(layer, carry):
        for what, p, ahead in repeat:
            if ahead:

                @pl.when(layer < layers - 1)
                def _():
                    step(what, p, jnp.minimum(layer + 1, layers - 1))
            else:
                step(what, p, layer)
        return carry

    lax.fori_loop(0, layers, one_layer, 0)

    at_d = pl.ds(pl.multiple_of(me * local_d, LANES), local_d)
    gain = out_gain[layers - 1, :, at_d]
    shift = out_shift[layers - 1, :, at_d]
    for p in range(chunks):
        for copy in stat_copies(p):
            copy.wait_recv()
        stats = jnp.transpose(st_recv[p])[:CHUNK]
        total = stats[:, 0:1]
        for s in range(1, n):
            total = total + stats[:, 8 * s : 8 * s + 1]
        mean = total * (1.0 / width)
        spread = jnp.zeros_like(mean)
        for s in range(n):
            off = stats[:, 8 * s : 8 * s + 1] * (1.0 / local_d) - mean
            spread = spread + stats[:, 8 * s + 1 : 8 * s + 2] + off * off * local_d
        scale = lax.rsqrt(spread * (1.0 / width) + EPS)
        span = pl.ds(starts[p], CHUNK)
        out[span, :] = ((zf[span, :] - mean) * scale * gain + shift).astype(jnp.bfloat16)

    def drain_layer(layer, carry):
        for p in range(chunks):
            drain(hbuf, layer, 0, p)
            drain(cbuf, layer, 1, p)
        for e in range(2):
            on(halo_copy(layer, e), "wait_send")
        return carry

    lax.fori_loop(0, layers, drain_layer, 0)
    for p in range(chunks):
        for copy in stat_copies(p):
            copy.wait_send()


def on_device(
    n,
    n_sp,
    stream,
    doc_ids,
    w_value,
    w_gate,
    conv_kernel,
    conv_gain,
    conv_shift,
    w_proj,
    out_gain,
    out_shift,
):
    rows, local_d = stream.shape
    layers, width, local_c = w_value.shape
    chunks = rows // CHUNK
    first, repeat = plan(chunks)
    docs = jnp.broadcast_to(doc_ids[:, None], (rows, LANES))
    vmem = pl.BlockSpec(memory_space=pltpu.VMEM)
    hbm = pl.BlockSpec(memory_space=pl.ANY)
    ways = 6 if n == 4 else n - 1
    dma = pltpu.SemaphoreType.DMA
    return pl.pallas_call(
        functools.partial(kernel, n, n_sp, first, repeat),
        out_shape=jax.ShapeDtypeStruct((rows, local_d), jnp.bfloat16),
        in_specs=[vmem, vmem, hbm, hbm, vmem, vmem, vmem, hbm, vmem, vmem],
        out_specs=vmem,
        scratch_shapes=[
            pltpu.VMEM((layers, 1, width), jnp.float32),
            pltpu.VMEM((layers, 1, width), jnp.float32),
            pltpu.VMEM((layers, 1, width), jnp.float32),
            pltpu.VMEM((layers, 1, width), jnp.float32),
            pltpu.VMEM((layers, width, local_c), jnp.bfloat16),
            pltpu.VMEM((layers, width, local_c), jnp.bfloat16),
            pltpu.VMEM((layers, local_c * n, local_d), jnp.bfloat16),
            pltpu.VMEM((layers, n, rows, local_d), jnp.bfloat16),
            pltpu.VMEM((layers, n, rows, local_c), jnp.bfloat16),
            pltpu.VMEM((rows, n * local_d), jnp.bfloat16),
            pltpu.VMEM((CHUNK, n * local_c), jnp.bfloat16),
            pltpu.VMEM((layers, local_c // LANES, rows + 2 * PAD, LANES), jnp.float32),
            pltpu.VMEM((rows + 2 * PAD, LANES), jnp.int32),
            pltpu.VMEM((layers, 32, local_c), jnp.float32),
            pltpu.VMEM((rows, local_d), jnp.float32),
            pltpu.VMEM((chunks, 8, LANES), jnp.float32),
            pltpu.VMEM((chunks, LANES, LANES), jnp.float32),
            pltpu.VMEM((CHUNK, LANES), jnp.float32),
            pltpu.VMEM((CHUNK, LANES), jnp.float32),
            dma((3, layers)),
            dma((2 * layers, chunks, ways)),
            dma((2 * layers, chunks, ways)),
            dma((layers, 2)),
            dma((layers, 2)),
            dma((2,)),
            dma((2,)),
            dma((chunks, n - 1)),
            dma((chunks, n - 1)),
        ],
        compiler_params=pltpu.CompilerParams(
            collective_id=0, has_side_effects=True, vmem_limit_bytes=60 * 1024 * 1024
        ),
        name="conv_stack",
    )(
        stream,
        docs,
        w_value,
        w_gate,
        conv_kernel,
        conv_gain,
        conv_shift,
        w_proj,
        out_gain,
        out_shift,
    )


def solution(mesh):
    in_specs = (
        P("sp", "tp"),
        P("sp"),
        P(None, None, "tp"),
        P(None, None, "tp"),
        P(None, None, "tp"),
        P(),
        P(),
        P(None, None, "tp"),
        P(),
        P(),
    )
    return jax.shard_map(
        functools.partial(on_device, mesh.shape["tp"], mesh.shape["sp"]),
        mesh=mesh,
        in_specs=in_specs,
        out_specs=P("sp", "tp"),
        check_vma=False,
    )
```

```python
import functools

import jax
import jax.numpy as jnp
from jax import lax
from jax.experimental import pallas as pl
from jax.experimental.pallas import tpu as pltpu
from jax.sharding import PartitionSpec as P

KERNEL = 31
HALF = 15
PAD = 16
LANES = 128
ROW_BLOCK = 16
CONV_BLOCK = 32
SUM_BLOCK = 32
ALPHA = 2.0**0.25
EPS = 1e-05
MESH = pl.DeviceIdType.MESH


SIZES = (64, 96, 64, 96, 64)
DIRECT = ((1, 4),)
FIRST = (
    ("send", 0),
    ("send", 1),
    ("hr0", 0),
    ("hr1", 0),
    ("send", 2),
    ("hr0", 1),
    ("hr1", 1),
    ("send", 3),
    ("hr0", 2),
    ("glu", 0),
    ("hr1", 2),
    ("send", 4),
    ("docs", 0),
    ("glu", 1),
    ("hr1", 3),
)
REPEAT = (
    ("hr0", 3, 0),
    ("conv", 0, 0),
    ("glu", 2, 0),
    ("hr1", 4, 0),
    ("hr0", 4, 0),
    ("conv", 1, 0),
    ("glu", 3, 0),
    ("cr1", 0, 0),
    ("cr0", 0, 0),
    ("conv", 2, 0),
    ("glu", 4, 0),
    ("cr0", 1, 0),
    ("cr1", 1, 0),
    ("conv", 3, 0),
    ("proj", 0, 0),
    ("cr1", 2, 0),
    ("cr0", 2, 0),
    ("cr1", 3, 0),
    ("cr0", 3, 0),
    ("conv", 4, 0),
    ("proj", 1, 0),
    ("hr0", 0, 1),
    ("hr1", 0, 1),
    ("proj", 2, 0),
    ("cr0", 4, 0),
    ("cr1", 4, 0),
    ("hr0", 1, 1),
    ("hr1", 1, 1),
    ("proj", 3, 0),
    ("hr0", 2, 1),
    ("glu", 0, 1),
    ("hr1", 2, 1),
    ("proj", 4, 0),
    ("glu", 1, 1),
    ("hr1", 3, 1),
)


def split(rows):
    return SIZES if sum(SIZES) == rows else (96,) * (rows // 96)


def plan(chunks):
    if chunks == len(SIZES):
        return FIRST, REPEAT
    first = [("send", p) for p in range(chunks)] + [("docs", 0)]
    repeat = [("hr%d" % i, p, 0) for p in range(chunks) for i in range(2)]
    repeat += [("glu", p, 0) for p in range(chunks)]
    repeat += [("conv", p, 0) for p in range(chunks)]
    repeat += [("cr%d" % i, p, 0) for p in range(chunks) for i in range(2)]
    repeat += [("proj", p, 0) for p in range(chunks)]
    return first, repeat


def sigmoid(v):
    return 0.5 * jnp.tanh(0.5 * v) + 0.5


def silu_of_half(u):
    return u * jnp.tanh(u) + u


def kernel(
    n,
    n_sp,
    first,
    repeat,
    stream,
    docs_hbm,
    wv_hbm,
    wg_hbm,
    taps_hbm,
    conv_gain_hbm,
    conv_shift_hbm,
    wp_hbm,
    out_gain_hbm,
    out_shift_hbm,
    out,
    docs,
    taps_in,
    conv_gain_in,
    conv_shift_in,
    out_gain_in,
    out_shift_in,
    conv_gain,
    conv_shift,
    out_gain,
    out_shift,
    wv,
    wg,
    wp,
    hbuf,
    cbuf,
    hn,
    act,
    glu,
    docpad,
    taps,
    zf,
    st_send,
    st_recv,
    means,
    scales,
    in_sem,
    w_sem,
    s_sem,
    r_sem,
    hs_sem,
    hr_sem,
    ds_sem,
    dr_sem,
    ss_sem,
    sr_sem,
):
    rows, local_d = stream.shape
    layers, width, local_c = wv.shape
    groups = local_c // LANES
    sizes = split(rows)
    chunks = len(sizes)
    ends = [sum(sizes[: p + 1]) for p in range(chunks)]
    relayed = n == 4
    me = lax.axis_index("tp")
    sp = lax.axis_index("sp")
    parity = lax.rem(sp, 2)

    def wait_weight(i, layer):
        src, dst = ((wv_hbm, wv), (wg_hbm, wg), (wp_hbm, wp))[i]
        pltpu.make_async_copy(src.at[layer], dst.at[layer], w_sem.at[i, layer]).wait()

    barrier = pltpu.get_barrier_semaphore()
    for j in range(1, n):
        pl.semaphore_signal(
            barrier, inc=1, device_id={"tp": lax.rem(me + j, n)}, device_id_type=MESH
        )

    @pl.when(sp > 0)
    def _():
        pl.semaphore_signal(barrier, inc=1, device_id={"sp": sp - 1}, device_id_type=MESH)

    @pl.when(sp < n_sp - 1)
    def _():
        pl.semaphore_signal(barrier, inc=1, device_id={"sp": sp + 1}, device_id_type=MESH)

    loads = [
        pltpu.make_async_copy(src, dst, in_sem.at[i])
        for i, (src, dst) in enumerate(
            (
                (stream, hbuf.at[0, me]),
                (docs_hbm, docs),
                (taps_hbm, taps_in),
                (conv_gain_hbm, conv_gain_in),
                (conv_shift_hbm, conv_shift_in),
                (out_gain_hbm, out_gain_in),
                (out_shift_hbm, out_shift_in),
            )
        )
    ]
    for load in loads[:2]:
        load.start()
    for layer in range(layers):
        for i, (src, dst) in enumerate(((wv_hbm, wv), (wg_hbm, wg), (wp_hbm, wp))):
            pltpu.make_async_copy(src.at[layer], dst.at[layer], w_sem.at[i, layer]).start()
    for load in loads[2:]:
        load.start()

    st_send[...] = jnp.zeros((chunks, 8, LANES), jnp.float32)
    st_recv[...] = jnp.zeros((chunks, LANES, LANES), jnp.float32)

    @pl.when(sp == 0)
    def _():
        docpad[pl.ds(0, PAD), :] = jnp.full((PAD, LANES), -1, jnp.int32)
        glu[:, :, pl.ds(0, PAD), :] = jnp.zeros((layers, groups, PAD, LANES), jnp.float32)

    @pl.when(sp == n_sp - 1)
    def _():
        docpad[pl.ds(PAD + rows, PAD), :] = jnp.full((PAD, LANES), -1, jnp.int32)
        glu[:, :, pl.ds(PAD + rows, PAD), :] = jnp.zeros(
            (layers, groups, PAD, LANES), jnp.float32
        )

    beside = (sp > 0).astype(jnp.int32) + (sp < n_sp - 1).astype(jnp.int32)
    pl.semaphore_wait(barrier, n - 1 + beside)
    loads[0].wait()

    def first_row(p):
        return pl.multiple_of(ends[p] - sizes[p] + parity * (rows + sizes[p] - 2 * ends[p]), 32)

    starts = [first_row(p) for p in range(chunks)]

    if relayed:
        near_x = me + 1 - 2 * lax.rem(me, 2)
        near_y = me + 2 - 4 * (me // 2)

    def own_copies(buf, layer, kind, p):
        a = 2 * layer + kind
        half = sizes[p] // 2
        if relayed:
            plan = [(near_x, 0, 0), (near_y, half, 1), (near_x, half, 4), (near_y, 0, 5)]
            size = half
        else:
            plan = [(lax.rem(me + j, n), 0, j - 1) for j in range(1, n)]
            size = sizes[p]
        copies = []
        for peer, offset, i in plan:
            part = pl.ds(pl.multiple_of(starts[p] + offset, 16), size)
            block = buf.at[layer, me, part, :]
            copies.append(
                pltpu.make_async_remote_copy(
                    src_ref=block,
                    dst_ref=block,
                    send_sem=s_sem.at[a, p, i],
                    recv_sem=r_sem.at[a, p, i],
                    device_id={"tp": peer},
                    device_id_type=MESH,
                )
            )
        return copies

    def relay_copies(buf, layer, kind, p):
        a = 2 * layer + kind
        half = sizes[p] // 2
        out_copies = []
        for i, (origin, target) in enumerate(((near_x, near_y), (near_y, near_x))):
            part = buf.at[
                layer, origin, pl.ds(pl.multiple_of(starts[p] + i * half, 16), half), :
            ]
            out_copies.append(
                pltpu.make_async_remote_copy(
                    src_ref=part,
                    dst_ref=part,
                    send_sem=s_sem.at[a, p, 2 + i],
                    recv_sem=r_sem.at[a, p, 2 + i],
                    device_id={"tp": target},
                    device_id_type=MESH,
                )
            )
        return out_copies

    def send(buf, layer, kind, p):
        for copy in own_copies(buf, layer, kind, p):
            copy.start()
        maybe, when = routed(layer, kind, p)
        if maybe:

            @pl.when(when)
            def _():
                for copy in far_copies(buf, layer, kind, p):
                    copy.start()

    def routed(layer, kind, p):
        return relayed and (kind, p) in DIRECT, layer == layers - 1

    def far_copies(buf, layer, kind, p):
        a = 2 * layer + kind
        half = sizes[p] // 2
        copies = []
        for i in range(2):
            part = buf.at[
                layer, me, pl.ds(pl.multiple_of(starts[p] + i * half, 16), half), :
            ]
            copies.append(
                pltpu.make_async_remote_copy(
                    src_ref=part,
                    dst_ref=part,
                    send_sem=s_sem.at[a, p, 2 + i],
                    recv_sem=r_sem.at[a, p, 2 + i],
                    device_id={"tp": 3 - me},
                    device_id_type=MESH,
                )
            )
        return copies

    def relay(buf, layer, kind, p, i):
        if relayed:
            own_copies(buf, layer, kind, p)[i].wait_recv()
            maybe, when = routed(layer, kind, p)
            if maybe:

                @pl.when(jnp.logical_not(when))
                def _():
                    relay_copies(buf, layer, kind, p)[i].start()
            else:
                relay_copies(buf, layer, kind, p)[i].start()

    def finish(buf, layer, kind, p):
        if relayed:
            for copy in own_copies(buf, layer, kind, p)[2:] + relay_copies(buf, layer, kind, p):
                copy.wait_recv()
        else:
            for copy in own_copies(buf, layer, kind, p):
                copy.wait_recv()

    def drain(buf, layer, kind, p):
        for copy in own_copies(buf, layer, kind, p):
            copy.wait_send()
        if relayed:
            for copy in relay_copies(buf, layer, kind, p):
                copy.wait_send()

    def edge(e):
        side = lax.rem(parity + e, 2)
        partner = sp - 1 + 2 * side
        there = (partner >= 0) & (partner < n_sp)
        src = pl.multiple_of(PAD + side * (rows - PAD), PAD)
        dst = pl.multiple_of((1 - side) * (PAD + rows), PAD)
        return partner, there, src, dst

    def halo_copy(layer, e):
        partner, there, src, dst = edge(e)
        return there, pltpu.make_async_remote_copy(
            src_ref=glu.at[layer, :, pl.ds(src, PAD), :],
            dst_ref=glu.at[layer, :, pl.ds(dst, PAD), :],
            send_sem=hs_sem.at[layer, e],
            recv_sem=hr_sem.at[layer, e],
            device_id={"sp": partner},
            device_id_type=MESH,
        )

    def doc_copy(e):
        partner, there, src, dst = edge(e)
        return there, pltpu.make_async_remote_copy(
            src_ref=docpad.at[pl.ds(src, PAD), :],
            dst_ref=docpad.at[pl.ds(dst, PAD), :],
            send_sem=ds_sem.at[e],
            recv_sem=dr_sem.at[e],
            device_id={"sp": partner},
            device_id_type=MESH,
        )

    def on(pair, what):
        there, copy = pair

        @pl.when(there)
        def _():
            getattr(copy, what)()

    def normalize(size, load, store, gain, shift, piece, finish_with):
        lanes = range(piece // LANES)

        count = width // LANES

        def measure(i, carry):
            at = pl.multiple_of(i * SUM_BLOCK, SUM_BLOCK)
            pivot = None
            for s in range(n):
                part = load(s, at, SUM_BLOCK)
                for g in lanes:
                    value = part[:, g * LANES : (g + 1) * LANES].astype(jnp.float32)
                    if pivot is None:
                        pivot = value
                        first = jnp.zeros_like(value)
                        second = jnp.zeros_like(value)
                    else:
                        off = value - pivot
                        first = first + off
                        second = second + off * off
            middle = first * (1.0 / count)
            means[pl.ds(at, SUM_BLOCK), :] = pivot + middle
            scales[pl.ds(at, SUM_BLOCK), :] = jnp.maximum(second - first * middle, 0.0)
            return carry

        lax.fori_loop(0, size // SUM_BLOCK, measure, 0, unroll=True)
        every = pl.ds(0, size)
        middle = means[every, :]
        mean = jnp.sum(middle, axis=1, keepdims=True) * (1.0 / LANES)
        off = middle - mean
        spread = jnp.sum(scales[every, :] + off * off * count, axis=1, keepdims=True)
        means[every, :] = jnp.broadcast_to(mean, (size, LANES))
        scales[every, :] = jnp.broadcast_to(
            lax.rsqrt(spread * (1.0 / width) + EPS), (size, LANES)
        )

        def body(i, carry):
            at = pl.multiple_of(i * ROW_BLOCK, ROW_BLOCK)
            mean = means[pl.ds(at, ROW_BLOCK), :]
            scale = scales[pl.ds(at, ROW_BLOCK), :]
            for s in range(n):
                part = load(s, at, ROW_BLOCK)
                for g in lanes:
                    value = part[:, g * LANES : (g + 1) * LANES].astype(jnp.float32)
                    column = s * piece + g * LANES
                    value = (value - mean) * scale * gain(column) + shift(column)
                    store(s, at, g * LANES, finish_with(value).astype(jnp.bfloat16))
            return carry

        lax.fori_loop(0, size // ROW_BLOCK, body, 0, unroll=True)

    def make_glu(layer, p):
        r0 = starts[p]
        size = sizes[p]
        span = pl.ds(r0, size)

        @pl.when(layer == 0)
        def _():
            for s in range(n):
                hn[span, pl.ds(s * local_d, local_d)] = hbuf[0, s, span, :]

        @pl.when(layer > 0)
        def _():
            before = jnp.maximum(layer - 1, 0)
            normalize(
                size,
                lambda s, at, count: hbuf[layer, s, pl.ds(r0 + at, count), :],
                lambda s, at, c, v: hn.__setitem__(
                    (pl.ds(r0 + at, ROW_BLOCK), pl.ds(s * local_d + c, LANES)), v
                ),
                lambda c: out_gain[before, :, pl.ds(c, LANES)],
                lambda c: out_shift[before, :, pl.ds(c, LANES)],
                local_d,
                lambda v: v,
            )

        x = hn[span, :]
        lin = jnp.dot(x, wv[layer], preferred_element_type=jnp.float32)
        gat = jnp.dot(x, wg[layer], preferred_element_type=jnp.float32)
        gated = (lin * sigmoid(gat)).astype(jnp.bfloat16).astype(jnp.float32)
        at = pl.multiple_of(r0 + PAD, PAD)
        for g in range(groups):
            glu[layer, g, pl.ds(at, size), :] = gated[:, g * LANES : (g + 1) * LANES]

    def convolve(layer, p):
        r0 = starts[p]

        def body(i, carry):
            t0 = pl.multiple_of(r0 + i * CONV_BLOCK, CONV_BLOCK)
            centre = docpad[pl.ds(t0 + PAD, CONV_BLOCK), :]
            totals = [jnp.zeros((CONV_BLOCK, LANES), jnp.float32) for _ in range(groups)]
            for k in range(KERNEL):
                at = pl.ds(t0 + k + PAD - HALF, CONV_BLOCK)
                keep = docpad[at, :] == centre
                for g in range(groups):
                    tap = taps[layer, pl.ds(k, 1), pl.ds(g * LANES, LANES)]
                    totals[g] = totals[g] + jnp.where(keep, glu[layer, g, at, :], 0.0) * tap
            for g in range(groups):
                cbuf[layer, me, pl.ds(t0, CONV_BLOCK), pl.ds(g * LANES, LANES)] = totals[
                    g
                ].astype(jnp.bfloat16)
            return carry

        lax.fori_loop(0, sizes[p] // CONV_BLOCK, body, 0)

    def project(layer, p):
        r0 = starts[p]
        size = sizes[p]
        span = pl.ds(r0, size)
        normalize(
            size,
            lambda s, at, count: cbuf[layer, s, pl.ds(r0 + at, count), :],
            lambda s, at, c, v: act.__setitem__(
                (pl.ds(at, ROW_BLOCK), pl.ds(s * local_c + c, LANES)), v
            ),
            lambda c: conv_gain[layer, :, pl.ds(c, LANES)],
            lambda c: conv_shift[layer, :, pl.ds(c, LANES)],
            local_c,
            silu_of_half,
        )
        z = jnp.dot(act[pl.ds(0, size), :], wp[layer], preferred_element_type=jnp.float32)
        own = hn[span, pl.ds(pl.multiple_of(me * local_d, LANES), local_d)]
        z = z + ALPHA * own.astype(jnp.float32)

        @pl.when(layer < layers - 1)
        def _():
            after = jnp.minimum(layer + 1, layers - 1)
            hbuf[after, me, span, :] = z.astype(jnp.bfloat16)
            send(hbuf, after, 0, p)

        @pl.when(layer == layers - 1)
        def _():
            zf[span, :] = z
            total = jnp.sum(z, axis=1, keepdims=True)
            off = z - total * (1.0 / local_d)
            spread = jnp.sum(off * off, axis=1, keepdims=True)
            lane = lax.broadcasted_iota(jnp.int32, (size, LANES), 1)
            tile = jnp.where(lane == 0, total, jnp.where(lane == 1, spread, 0.0))
            stats = jnp.transpose(tile)[:8, :]
            st_send[p, :, pl.ds(0, size)] = stats
            st_recv[p, pl.ds(pl.multiple_of(me * 8, 8), 8), pl.ds(0, size)] = stats
            for copy in stat_copies(p):
                copy.start()

    def stat_copies(p):
        return [
            pltpu.make_async_remote_copy(
                src_ref=st_send.at[p],
                dst_ref=st_recv.at[p, pl.ds(pl.multiple_of(me * 8, 8), 8), :],
                send_sem=ss_sem.at[p, j - 1],
                recv_sem=sr_sem.at[p, j - 1],
                device_id={"tp": lax.rem(me + j, n)},
                device_id_type=MESH,
            )
            for j in range(1, n)
        ]

    def prepare():
        loads[1].wait()
        for i in range(rows // LANES):
            row = jnp.broadcast_to(docs[pl.ds(i, 1), :], (LANES, LANES))
            docpad[pl.ds(PAD + i * LANES, LANES), :] = jnp.transpose(row)
        for e in range(2):
            on(doc_copy(e), "start")
        for load in loads[2:]:
            load.wait()
        taps[:, pl.ds(0, KERNEL), :] = taps_in[...].astype(jnp.float32)
        for layer in range(layers):
            conv_gain[layer] = 0.5 * conv_gain_in[pl.ds(layer, 1), :]
            conv_shift[layer] = 0.5 * conv_shift_in[pl.ds(layer, 1), :]
            out_gain[layer] = out_gain_in[pl.ds(layer, 1), :]
            out_shift[layer] = out_shift_in[pl.ds(layer, 1), :]

    def step(what, p, layer):
        if what == "send":
            send(hbuf, 0, 0, p)
        elif what in ("hr0", "hr1"):
            relay(hbuf, layer, 0, p, int(what[2]))
        elif what in ("cr0", "cr1"):
            relay(cbuf, layer, 1, p, int(what[2]))
        elif what == "glu":
            finish(hbuf, layer, 0, p)
            if p == 0:
                wait_weight(0, layer)
                wait_weight(1, layer)
            make_glu(layer, p)
            if p == 0:
                on(halo_copy(layer, 0), "start")
            if p == chunks - 1:
                on(halo_copy(layer, 1), "start")
        elif what == "conv":
            if p == 0:
                on(halo_copy(layer, 0), "wait_recv")
            if p == chunks - 1:
                on(halo_copy(layer, 1), "wait_recv")
            convolve(layer, p)
            send(cbuf, layer, 1, p)
        elif what == "proj":
            if p == 0:
                wait_weight(2, layer)
            finish(cbuf, layer, 1, p)
            project(layer, p)

    for what, p in first:
        if what == "docs":
            prepare()
        else:
            step(what, p, 0)

    def one_layer(layer, carry):
        for what, p, ahead in repeat:
            if ahead:

                @pl.when(layer < layers - 1)
                def _():
                    step(what, p, jnp.minimum(layer + 1, layers - 1))
            else:
                step(what, p, layer)
        return carry

    for e in range(2):
        on(doc_copy(e), "wait_recv")
    lax.fori_loop(0, layers, one_layer, 0)

    at_d = pl.ds(pl.multiple_of(me * local_d, LANES), local_d)
    gain = out_gain[layers - 1, :, at_d]
    shift = out_shift[layers - 1, :, at_d]
    for p in range(chunks):
        for copy in stat_copies(p):
            copy.wait_recv()
        stats = jnp.transpose(st_recv[p])[: sizes[p]]
        total = stats[:, 0:1]
        for s in range(1, n):
            total = total + stats[:, 8 * s : 8 * s + 1]
        mean = total * (1.0 / width)
        spread = jnp.zeros_like(mean)
        for s in range(n):
            off = stats[:, 8 * s : 8 * s + 1] * (1.0 / local_d) - mean
            spread = spread + stats[:, 8 * s + 1 : 8 * s + 2] + off * off * local_d
        scale = lax.rsqrt(spread * (1.0 / width) + EPS)
        span = pl.ds(starts[p], sizes[p])
        out[span, :] = ((zf[span, :] - mean) * scale * gain + shift).astype(jnp.bfloat16)

    def drain_layer(layer, carry):
        for p in range(chunks):
            drain(hbuf, layer, 0, p)
            drain(cbuf, layer, 1, p)
        for e in range(2):
            on(halo_copy(layer, e), "wait_send")
        return carry

    lax.fori_loop(0, layers, drain_layer, 0)
    for e in range(2):
        on(doc_copy(e), "wait_send")
    for p in range(chunks):
        for copy in stat_copies(p):
            copy.wait_send()


def on_device(
    n,
    n_sp,
    stream,
    doc_ids,
    w_value,
    w_gate,
    conv_kernel,
    conv_gain,
    conv_shift,
    w_proj,
    out_gain,
    out_shift,
):
    rows, local_d = stream.shape
    layers, width, local_c = w_value.shape
    sizes = split(rows)
    chunks, tall = len(sizes), max(sizes)
    first, repeat = plan(chunks)
    docs = doc_ids.reshape(rows // LANES, LANES)
    vmem = pl.BlockSpec(memory_space=pltpu.VMEM)
    hbm = pl.BlockSpec(memory_space=pl.ANY)
    ways = 6 if n == 4 else n - 1
    dma = pltpu.SemaphoreType.DMA
    return pl.pallas_call(
        functools.partial(kernel, n, n_sp, first, repeat),
        out_shape=jax.ShapeDtypeStruct((rows, local_d), jnp.bfloat16),
        in_specs=[hbm] * 10,
        out_specs=vmem,
        scratch_shapes=[
            pltpu.VMEM(docs.shape, jnp.int32),
            pltpu.VMEM(conv_kernel.shape, jnp.bfloat16),
            pltpu.VMEM((layers, width), jnp.float32),
            pltpu.VMEM((layers, width), jnp.float32),
            pltpu.VMEM((layers, width), jnp.float32),
            pltpu.VMEM((layers, width), jnp.float32),
            pltpu.VMEM((layers, 1, width), jnp.float32),
            pltpu.VMEM((layers, 1, width), jnp.float32),
            pltpu.VMEM((layers, 1, width), jnp.float32),
            pltpu.VMEM((layers, 1, width), jnp.float32),
            pltpu.VMEM((layers, width, local_c), jnp.bfloat16),
            pltpu.VMEM((layers, width, local_c), jnp.bfloat16),
            pltpu.VMEM((layers, local_c * n, local_d), jnp.bfloat16),
            pltpu.VMEM((layers, n, rows, local_d), jnp.bfloat16),
            pltpu.VMEM((layers, n, rows, local_c), jnp.bfloat16),
            pltpu.VMEM((rows, n * local_d), jnp.bfloat16),
            pltpu.VMEM((tall, n * local_c), jnp.bfloat16),
            pltpu.VMEM((layers, local_c // LANES, rows + 2 * PAD, LANES), jnp.float32),
            pltpu.VMEM((rows + 2 * PAD, LANES), jnp.int32),
            pltpu.VMEM((layers, 32, local_c), jnp.float32),
            pltpu.VMEM((rows, local_d), jnp.float32),
            pltpu.VMEM((chunks, 8, LANES), jnp.float32),
            pltpu.VMEM((chunks, LANES, LANES), jnp.float32),
            pltpu.VMEM((tall, LANES), jnp.float32),
            pltpu.VMEM((tall, LANES), jnp.float32),
            dma((7,)),
            dma((3, layers)),
            dma((2 * layers, chunks, ways)),
            dma((2 * layers, chunks, ways)),
            dma((layers, 2)),
            dma((layers, 2)),
            dma((2,)),
            dma((2,)),
            dma((chunks, n - 1)),
            dma((chunks, n - 1)),
        ],
        compiler_params=pltpu.CompilerParams(
            collective_id=0, has_side_effects=True, vmem_limit_bytes=60 * 1024 * 1024
        ),
        name="conv_stack",
    )(
        stream,
        docs,
        w_value,
        w_gate,
        conv_kernel,
        conv_gain,
        conv_shift,
        w_proj,
        out_gain,
        out_shift,
    )


def solution(mesh):
    in_specs = (
        P("sp", "tp"),
        P("sp"),
        P(None, None, "tp"),
        P(None, None, "tp"),
        P(None, None, "tp"),
        P(),
        P(),
        P(None, None, "tp"),
        P(),
        P(),
    )
    return jax.shard_map(
        functools.partial(on_device, mesh.shape["tp"], mesh.shape["sp"]),
        mesh=mesh,
        in_specs=in_specs,
        out_specs=P("sp", "tp"),
        check_vma=False,
    )
```

```python
import functools

import jax
import jax.numpy as jnp
from jax import lax
from jax.experimental import pallas as pl
from jax.experimental.pallas import tpu as pltpu
from jax.sharding import PartitionSpec as P

KERNEL = 31
HALF = 15
PAD = 16
LANES = 128
ROW_BLOCK = 16
CONV_BLOCK = 32
SUM_BLOCK = 32
ALPHA = 2.0**0.25
EPS = 1e-05
MESH = pl.DeviceIdType.MESH


SIZES = (64, 96, 64, 96, 64)
DIRECT = ()
FIRST = (
    ("send", 0),
    ("send", 1),
    ("send", 2),
    ("hr1", 0),
    ("hr0", 0),
    ("hr1", 1),
    ("hr0", 1),
    ("hr1", 2),
    ("send", 3),
    ("hr0", 2),
    ("glu", 0),
    ("send", 4),
    ("docs", 0),
)
REPEAT = (
    ("glu", 1, 0),
    ("hr0", 3, 0),
    ("hr1", 3, 0),
    ("conv", 0, 0),
    ("glu", 2, 0),
    ("hr1", 4, 0),
    ("hr0", 4, 0),
    ("conv", 1, 0),
    ("glu", 3, 0),
    ("conv", 2, 0),
    ("glu", 4, 0),
    ("cr1", 1, 0),
    ("cr1", 0, 0),
    ("cr0", 1, 0),
    ("cr0", 0, 0),
    ("conv", 3, 0),
    ("conv", 4, 0),
    ("proj", 1, 0),
    ("proj", 0, 0),
    ("cr1", 2, 0),
    ("cr0", 2, 0),
    ("cr1", 3, 0),
    ("hr1", 1, 1),
    ("cr0", 3, 0),
    ("hr1", 0, 1),
    ("hr0", 0, 1),
    ("hr0", 1, 1),
    ("cr0", 4, 0),
    ("cr1", 4, 0),
    ("proj", 2, 0),
    ("proj", 3, 0),
    ("glu", 0, 1),
    ("hr1", 2, 1),
    ("hr0", 2, 1),
    ("proj", 4, 0),
)


def split(rows):
    return SIZES if sum(SIZES) == rows else (96,) * (rows // 96)


def plan(chunks):
    if chunks == len(SIZES):
        return FIRST, REPEAT
    first = [("send", p) for p in range(chunks)] + [("docs", 0)]
    repeat = [("hr%d" % i, p, 0) for p in range(chunks) for i in range(2)]
    repeat += [("glu", p, 0) for p in range(chunks)]
    repeat += [("conv", p, 0) for p in range(chunks)]
    repeat += [("cr%d" % i, p, 0) for p in range(chunks) for i in range(2)]
    repeat += [("proj", p, 0) for p in range(chunks)]
    return first, repeat


def sigmoid(v):
    return 0.5 * jnp.tanh(0.5 * v) + 0.5


def silu_of_half(u):
    return u * jnp.tanh(u) + u


def kernel(
    n,
    n_sp,
    first,
    repeat,
    stream,
    docs_hbm,
    wv_hbm,
    wg_hbm,
    taps_hbm,
    conv_gain_hbm,
    conv_shift_hbm,
    wp_hbm,
    out_gain_hbm,
    out_shift_hbm,
    out,
    docs,
    taps_in,
    conv_gain_in,
    conv_shift_in,
    out_gain_in,
    out_shift_in,
    conv_gain,
    conv_shift,
    out_gain,
    out_shift,
    wv,
    wg,
    wp,
    hbuf,
    cbuf,
    hn,
    act,
    glu,
    docpad,
    taps,
    zf,
    st_send,
    st_recv,
    means,
    scales,
    in_sem,
    w_sem,
    s_sem,
    r_sem,
    hs_sem,
    hr_sem,
    ds_sem,
    dr_sem,
    ss_sem,
    sr_sem,
):
    rows, local_d = stream.shape
    layers, width, local_c = wv.shape
    groups = local_c // LANES
    sizes = split(rows)
    chunks = len(sizes)
    ends = [sum(sizes[: p + 1]) for p in range(chunks)]
    relayed = n == 4
    me = lax.axis_index("tp")
    sp = lax.axis_index("sp")
    parity = lax.rem(sp, 2)

    def wait_weight(i, layer):
        src, dst = ((wv_hbm, wv), (wg_hbm, wg), (wp_hbm, wp))[i]
        pltpu.make_async_copy(src.at[layer], dst.at[layer], w_sem.at[i, layer]).wait()

    barrier = pltpu.get_barrier_semaphore()
    for j in range(1, n):
        pl.semaphore_signal(
            barrier, inc=1, device_id={"tp": lax.rem(me + j, n)}, device_id_type=MESH
        )

    @pl.when(sp > 0)
    def _():
        pl.semaphore_signal(barrier, inc=1, device_id={"sp": sp - 1}, device_id_type=MESH)

    @pl.when(sp < n_sp - 1)
    def _():
        pl.semaphore_signal(barrier, inc=1, device_id={"sp": sp + 1}, device_id_type=MESH)

    loads = [
        pltpu.make_async_copy(src, dst, in_sem.at[i])
        for i, (src, dst) in enumerate(
            (
                (stream, hbuf.at[0, me]),
                (docs_hbm, docs),
                (taps_hbm, taps_in),
                (conv_gain_hbm, conv_gain_in),
                (conv_shift_hbm, conv_shift_in),
                (out_gain_hbm, out_gain_in),
                (out_shift_hbm, out_shift_in),
            )
        )
    ]
    for load in loads[:2]:
        load.start()
    for layer in range(layers):
        for i, (src, dst) in enumerate(((wv_hbm, wv), (wg_hbm, wg), (wp_hbm, wp))):
            pltpu.make_async_copy(src.at[layer], dst.at[layer], w_sem.at[i, layer]).start()
    for load in loads[2:]:
        load.start()

    st_send[...] = jnp.zeros((chunks, 8, LANES), jnp.float32)
    st_recv[...] = jnp.zeros((chunks, LANES, LANES), jnp.float32)

    @pl.when(sp == 0)
    def _():
        docpad[pl.ds(0, PAD), :] = jnp.full((PAD, LANES), -1, jnp.int32)
        glu[:, :, pl.ds(0, PAD), :] = jnp.zeros((layers, groups, PAD, LANES), jnp.float32)

    @pl.when(sp == n_sp - 1)
    def _():
        docpad[pl.ds(PAD + rows, PAD), :] = jnp.full((PAD, LANES), -1, jnp.int32)
        glu[:, :, pl.ds(PAD + rows, PAD), :] = jnp.zeros(
            (layers, groups, PAD, LANES), jnp.float32
        )

    beside = (sp > 0).astype(jnp.int32) + (sp < n_sp - 1).astype(jnp.int32)
    pl.semaphore_wait(barrier, n - 1 + beside)
    loads[0].wait()

    def first_row(p):
        return pl.multiple_of(ends[p] - sizes[p] + parity * (rows + sizes[p] - 2 * ends[p]), 32)

    starts = [first_row(p) for p in range(chunks)]

    if relayed:
        near_x = me + 1 - 2 * lax.rem(me, 2)
        near_y = me + 2 - 4 * (me // 2)

    def own_copies(buf, layer, kind, p):
        a = 2 * layer + kind
        half = sizes[p] // 2
        if relayed:
            plan = [(near_x, 0, 0), (near_y, half, 1), (near_x, half, 4), (near_y, 0, 5)]
            size = half
        else:
            plan = [(lax.rem(me + j, n), 0, j - 1) for j in range(1, n)]
            size = sizes[p]
        copies = []
        for peer, offset, i in plan:
            part = pl.ds(pl.multiple_of(starts[p] + offset, 16), size)
            block = buf.at[layer, me, part, :]
            copies.append(
                pltpu.make_async_remote_copy(
                    src_ref=block,
                    dst_ref=block,
                    send_sem=s_sem.at[a, p, i],
                    recv_sem=r_sem.at[a, p, i],
                    device_id={"tp": peer},
                    device_id_type=MESH,
                )
            )
        return copies

    def relay_copies(buf, layer, kind, p):
        a = 2 * layer + kind
        half = sizes[p] // 2
        out_copies = []
        for i, (origin, target) in enumerate(((near_x, near_y), (near_y, near_x))):
            part = buf.at[
                layer, origin, pl.ds(pl.multiple_of(starts[p] + i * half, 16), half), :
            ]
            out_copies.append(
                pltpu.make_async_remote_copy(
                    src_ref=part,
                    dst_ref=part,
                    send_sem=s_sem.at[a, p, 2 + i],
                    recv_sem=r_sem.at[a, p, 2 + i],
                    device_id={"tp": target},
                    device_id_type=MESH,
                )
            )
        return out_copies

    def send(buf, layer, kind, p):
        for copy in own_copies(buf, layer, kind, p):
            copy.start()
        maybe, when = routed(layer, kind, p)
        if maybe:

            @pl.when(when)
            def _():
                for copy in far_copies(buf, layer, kind, p):
                    copy.start()

    def routed(layer, kind, p):
        return relayed and (kind, p) in DIRECT, layer == layers - 1

    def far_copies(buf, layer, kind, p):
        a = 2 * layer + kind
        half = sizes[p] // 2
        copies = []
        for i in range(2):
            part = buf.at[
                layer, me, pl.ds(pl.multiple_of(starts[p] + i * half, 16), half), :
            ]
            copies.append(
                pltpu.make_async_remote_copy(
                    src_ref=part,
                    dst_ref=part,
                    send_sem=s_sem.at[a, p, 2 + i],
                    recv_sem=r_sem.at[a, p, 2 + i],
                    device_id={"tp": 3 - me},
                    device_id_type=MESH,
                )
            )
        return copies

    def relay(buf, layer, kind, p, i):
        if relayed:
            own_copies(buf, layer, kind, p)[i].wait_recv()
            maybe, when = routed(layer, kind, p)
            if maybe:

                @pl.when(jnp.logical_not(when))
                def _():
                    relay_copies(buf, layer, kind, p)[i].start()
            else:
                relay_copies(buf, layer, kind, p)[i].start()

    def finish(buf, layer, kind, p):
        if relayed:
            for copy in own_copies(buf, layer, kind, p)[2:] + relay_copies(buf, layer, kind, p):
                copy.wait_recv()
        else:
            for copy in own_copies(buf, layer, kind, p):
                copy.wait_recv()

    def drain(buf, layer, kind, p):
        for copy in own_copies(buf, layer, kind, p):
            copy.wait_send()
        if relayed:
            for copy in relay_copies(buf, layer, kind, p):
                copy.wait_send()

    def edge(e):
        side = lax.rem(parity + e, 2)
        partner = sp - 1 + 2 * side
        there = (partner >= 0) & (partner < n_sp)
        src = pl.multiple_of(PAD + side * (rows - PAD), PAD)
        dst = pl.multiple_of((1 - side) * (PAD + rows), PAD)
        return partner, there, src, dst

    def halo_copy(layer, e):
        partner, there, src, dst = edge(e)
        return there, pltpu.make_async_remote_copy(
            src_ref=glu.at[layer, :, pl.ds(src, PAD), :],
            dst_ref=glu.at[layer, :, pl.ds(dst, PAD), :],
            send_sem=hs_sem.at[layer, e],
            recv_sem=hr_sem.at[layer, e],
            device_id={"sp": partner},
            device_id_type=MESH,
        )

    def doc_copy(e):
        partner, there, src, dst = edge(e)
        return there, pltpu.make_async_remote_copy(
            src_ref=docpad.at[pl.ds(src, PAD), :],
            dst_ref=docpad.at[pl.ds(dst, PAD), :],
            send_sem=ds_sem.at[e],
            recv_sem=dr_sem.at[e],
            device_id={"sp": partner},
            device_id_type=MESH,
        )

    def on(pair, what):
        there, copy = pair

        @pl.when(there)
        def _():
            getattr(copy, what)()

    def normalize(size, load, store, gain, shift, piece, finish_with):
        lanes = range(piece // LANES)

        count = width // LANES

        def measure(i, carry):
            at = pl.multiple_of(i * SUM_BLOCK, SUM_BLOCK)
            pivot = None
            for s in range(n):
                part = load(s, at, SUM_BLOCK)
                for g in lanes:
                    value = part[:, g * LANES : (g + 1) * LANES].astype(jnp.float32)
                    if pivot is None:
                        pivot = value
                        first = jnp.zeros_like(value)
                        second = jnp.zeros_like(value)
                    else:
                        off = value - pivot
                        first = first + off
                        second = second + off * off
            middle = first * (1.0 / count)
            means[pl.ds(at, SUM_BLOCK), :] = pivot + middle
            scales[pl.ds(at, SUM_BLOCK), :] = jnp.maximum(second - first * middle, 0.0)
            return carry

        lax.fori_loop(0, size // SUM_BLOCK, measure, 0, unroll=True)
        every = pl.ds(0, size)
        middle = means[every, :]
        mean = jnp.sum(middle, axis=1, keepdims=True) * (1.0 / LANES)
        off = middle - mean
        spread = jnp.sum(scales[every, :] + off * off * count, axis=1, keepdims=True)
        means[every, :] = jnp.broadcast_to(mean, (size, LANES))
        scales[every, :] = jnp.broadcast_to(
            lax.rsqrt(spread * (1.0 / width) + EPS), (size, LANES)
        )

        def body(i, carry):
            at = pl.multiple_of(i * ROW_BLOCK, ROW_BLOCK)
            mean = means[pl.ds(at, ROW_BLOCK), :]
            scale = scales[pl.ds(at, ROW_BLOCK), :]
            for s in range(n):
                part = load(s, at, ROW_BLOCK)
                for g in lanes:
                    value = part[:, g * LANES : (g + 1) * LANES].astype(jnp.float32)
                    column = s * piece + g * LANES
                    value = (value - mean) * scale * gain(column) + shift(column)
                    store(s, at, g * LANES, finish_with(value).astype(jnp.bfloat16))
            return carry

        lax.fori_loop(0, size // ROW_BLOCK, body, 0, unroll=True)

    def make_glu(layer, p):
        r0 = starts[p]
        size = sizes[p]
        span = pl.ds(r0, size)

        @pl.when(layer == 0)
        def _():
            for s in range(n):
                hn[span, pl.ds(s * local_d, local_d)] = hbuf[0, s, span, :]

        @pl.when(layer > 0)
        def _():
            before = jnp.maximum(layer - 1, 0)
            normalize(
                size,
                lambda s, at, count: hbuf[layer, s, pl.ds(r0 + at, count), :],
                lambda s, at, c, v: hn.__setitem__(
                    (pl.ds(r0 + at, ROW_BLOCK), pl.ds(s * local_d + c, LANES)), v
                ),
                lambda c: out_gain[before, :, pl.ds(c, LANES)],
                lambda c: out_shift[before, :, pl.ds(c, LANES)],
                local_d,
                lambda v: v,
            )

        x = hn[span, :]
        lin = jnp.dot(x, wv[layer], preferred_element_type=jnp.float32)
        gat = jnp.dot(x, wg[layer], preferred_element_type=jnp.float32)
        gated = (lin * sigmoid(gat)).astype(jnp.bfloat16).astype(jnp.float32)
        at = pl.multiple_of(r0 + PAD, PAD)
        for g in range(groups):
            glu[layer, g, pl.ds(at, size), :] = gated[:, g * LANES : (g + 1) * LANES]

    def convolve(layer, p):
        r0 = starts[p]

        def body(i, carry):
            t0 = pl.multiple_of(r0 + i * CONV_BLOCK, CONV_BLOCK)
            centre = docpad[pl.ds(t0 + PAD, CONV_BLOCK), :]
            totals = [jnp.zeros((CONV_BLOCK, LANES), jnp.float32) for _ in range(groups)]
            for k in range(KERNEL):
                at = pl.ds(t0 + k + PAD - HALF, CONV_BLOCK)
                keep = docpad[at, :] == centre
                for g in range(groups):
                    tap = taps[layer, pl.ds(k, 1), pl.ds(g * LANES, LANES)]
                    totals[g] = totals[g] + jnp.where(keep, glu[layer, g, at, :], 0.0) * tap
            for g in range(groups):
                cbuf[layer, me, pl.ds(t0, CONV_BLOCK), pl.ds(g * LANES, LANES)] = totals[
                    g
                ].astype(jnp.bfloat16)
            return carry

        lax.fori_loop(0, sizes[p] // CONV_BLOCK, body, 0)

    def project(layer, p):
        r0 = starts[p]
        size = sizes[p]
        span = pl.ds(r0, size)
        normalize(
            size,
            lambda s, at, count: cbuf[layer, s, pl.ds(r0 + at, count), :],
            lambda s, at, c, v: act.__setitem__(
                (pl.ds(at, ROW_BLOCK), pl.ds(s * local_c + c, LANES)), v
            ),
            lambda c: conv_gain[layer, :, pl.ds(c, LANES)],
            lambda c: conv_shift[layer, :, pl.ds(c, LANES)],
            local_c,
            silu_of_half,
        )
        z = jnp.dot(act[pl.ds(0, size), :], wp[layer], preferred_element_type=jnp.float32)
        own = hn[span, pl.ds(pl.multiple_of(me * local_d, LANES), local_d)]
        z = z + ALPHA * own.astype(jnp.float32)

        @pl.when(layer < layers - 1)
        def _():
            after = jnp.minimum(layer + 1, layers - 1)
            hbuf[after, me, span, :] = z.astype(jnp.bfloat16)
            send(hbuf, after, 0, p)

        @pl.when(layer == layers - 1)
        def _():
            zf[span, :] = z
            total = jnp.sum(z, axis=1, keepdims=True)
            off = z - total * (1.0 / local_d)
            spread = jnp.sum(off * off, axis=1, keepdims=True)
            lane = lax.broadcasted_iota(jnp.int32, (size, LANES), 1)
            tile = jnp.where(lane == 0, total, jnp.where(lane == 1, spread, 0.0))
            stats = jnp.transpose(tile)[:8, :]
            st_send[p, :, pl.ds(0, size)] = stats
            st_recv[p, pl.ds(pl.multiple_of(me * 8, 8), 8), pl.ds(0, size)] = stats
            for copy in stat_copies(p):
                copy.start()

    def stat_copies(p):
        return [
            pltpu.make_async_remote_copy(
                src_ref=st_send.at[p],
                dst_ref=st_recv.at[p, pl.ds(pl.multiple_of(me * 8, 8), 8), :],
                send_sem=ss_sem.at[p, j - 1],
                recv_sem=sr_sem.at[p, j - 1],
                device_id={"tp": lax.rem(me + j, n)},
                device_id_type=MESH,
            )
            for j in range(1, n)
        ]

    lead = [p for what, p, _ in repeat if what == "proj"][0]

    def prepare():
        loads[1].wait()
        for i in range(rows // LANES):
            row = jnp.broadcast_to(docs[pl.ds(i, 1), :], (LANES, LANES))
            docpad[pl.ds(PAD + i * LANES, LANES), :] = jnp.transpose(row)
        for e in range(2):
            on(doc_copy(e), "start")
        for load in loads[2:]:
            load.wait()
        taps[:, pl.ds(0, KERNEL), :] = taps_in[...].astype(jnp.float32)
        for layer in range(layers):
            conv_gain[layer] = 0.5 * conv_gain_in[pl.ds(layer, 1), :]
            conv_shift[layer] = 0.5 * conv_shift_in[pl.ds(layer, 1), :]
            out_gain[layer] = out_gain_in[pl.ds(layer, 1), :]
            out_shift[layer] = out_shift_in[pl.ds(layer, 1), :]

    def step(what, p, layer):
        if what == "send":
            send(hbuf, 0, 0, p)
        elif what in ("hr0", "hr1"):
            relay(hbuf, layer, 0, p, int(what[2]))
        elif what in ("cr0", "cr1"):
            relay(cbuf, layer, 1, p, int(what[2]))
        elif what == "glu":
            finish(hbuf, layer, 0, p)
            if p == 0:
                wait_weight(0, layer)
                wait_weight(1, layer)
            make_glu(layer, p)
            if p == 0:
                on(halo_copy(layer, 0), "start")
            if p == chunks - 1:
                on(halo_copy(layer, 1), "start")
        elif what == "conv":
            if p == 0:
                on(halo_copy(layer, 0), "wait_recv")
            if p == chunks - 1:
                on(halo_copy(layer, 1), "wait_recv")
            convolve(layer, p)
            send(cbuf, layer, 1, p)
        elif what == "proj":
            if p == lead:
                wait_weight(2, layer)
            finish(cbuf, layer, 1, p)
            project(layer, p)

    for what, p in first:
        if what == "docs":
            prepare()
        else:
            step(what, p, 0)

    def one_layer(layer, carry):
        for what, p, ahead in repeat:
            if ahead:

                @pl.when(layer < layers - 1)
                def _():
                    step(what, p, jnp.minimum(layer + 1, layers - 1))
            else:
                step(what, p, layer)
        return carry

    for e in range(2):
        on(doc_copy(e), "wait_recv")
    lax.fori_loop(0, layers, one_layer, 0)

    at_d = pl.ds(pl.multiple_of(me * local_d, LANES), local_d)
    gain = out_gain[layers - 1, :, at_d]
    shift = out_shift[layers - 1, :, at_d]
    for p in range(chunks):
        for copy in stat_copies(p):
            copy.wait_recv()
        stats = jnp.transpose(st_recv[p])[: sizes[p]]
        total = stats[:, 0:1]
        for s in range(1, n):
            total = total + stats[:, 8 * s : 8 * s + 1]
        mean = total * (1.0 / width)
        spread = jnp.zeros_like(mean)
        for s in range(n):
            off = stats[:, 8 * s : 8 * s + 1] * (1.0 / local_d) - mean
            spread = spread + stats[:, 8 * s + 1 : 8 * s + 2] + off * off * local_d
        scale = lax.rsqrt(spread * (1.0 / width) + EPS)
        span = pl.ds(starts[p], sizes[p])
        out[span, :] = ((zf[span, :] - mean) * scale * gain + shift).astype(jnp.bfloat16)

    def drain_layer(layer, carry):
        for p in range(chunks):
            drain(hbuf, layer, 0, p)
            drain(cbuf, layer, 1, p)
        for e in range(2):
            on(halo_copy(layer, e), "wait_send")
        return carry

    lax.fori_loop(0, layers, drain_layer, 0)
    for e in range(2):
        on(doc_copy(e), "wait_send")
    for p in range(chunks):
        for copy in stat_copies(p):
            copy.wait_send()


def on_device(
    n,
    n_sp,
    stream,
    doc_ids,
    w_value,
    w_gate,
    conv_kernel,
    conv_gain,
    conv_shift,
    w_proj,
    out_gain,
    out_shift,
):
    rows, local_d = stream.shape
    layers, width, local_c = w_value.shape
    sizes = split(rows)
    chunks, tall = len(sizes), max(sizes)
    first, repeat = plan(chunks)
    docs = doc_ids.reshape(rows // LANES, LANES)
    vmem = pl.BlockSpec(memory_space=pltpu.VMEM)
    hbm = pl.BlockSpec(memory_space=pl.ANY)
    ways = 6 if n == 4 else n - 1
    dma = pltpu.SemaphoreType.DMA
    return pl.pallas_call(
        functools.partial(kernel, n, n_sp, first, repeat),
        out_shape=pltpu.VMEM((rows, local_d), jnp.bfloat16),
        in_specs=[hbm] * 10,
        out_specs=vmem,
        scratch_shapes=[
            pltpu.VMEM(docs.shape, jnp.int32),
            pltpu.VMEM(conv_kernel.shape, jnp.bfloat16),
            pltpu.VMEM((layers, width), jnp.float32),
            pltpu.VMEM((layers, width), jnp.float32),
            pltpu.VMEM((layers, width), jnp.float32),
            pltpu.VMEM((layers, width), jnp.float32),
            pltpu.VMEM((layers, 1, width), jnp.float32),
            pltpu.VMEM((layers, 1, width), jnp.float32),
            pltpu.VMEM((layers, 1, width), jnp.float32),
            pltpu.VMEM((layers, 1, width), jnp.float32),
            pltpu.VMEM((layers, width, local_c), jnp.bfloat16),
            pltpu.VMEM((layers, width, local_c), jnp.bfloat16),
            pltpu.VMEM((layers, local_c * n, local_d), jnp.bfloat16),
            pltpu.VMEM((layers, n, rows, local_d), jnp.bfloat16),
            pltpu.VMEM((layers, n, rows, local_c), jnp.bfloat16),
            pltpu.VMEM((rows, n * local_d), jnp.bfloat16),
            pltpu.VMEM((tall, n * local_c), jnp.bfloat16),
            pltpu.VMEM((layers, local_c // LANES, rows + 2 * PAD, LANES), jnp.float32),
            pltpu.VMEM((rows + 2 * PAD, LANES), jnp.int32),
            pltpu.VMEM((layers, 32, local_c), jnp.float32),
            pltpu.VMEM((rows, local_d), jnp.float32),
            pltpu.VMEM((chunks, 8, LANES), jnp.float32),
            pltpu.VMEM((chunks, LANES, LANES), jnp.float32),
            pltpu.VMEM((tall, LANES), jnp.float32),
            pltpu.VMEM((tall, LANES), jnp.float32),
            dma((7,)),
            dma((3, layers)),
            dma((2 * layers, chunks, ways)),
            dma((2 * layers, chunks, ways)),
            dma((layers, 2)),
            dma((layers, 2)),
            dma((2,)),
            dma((2,)),
            dma((chunks, n - 1)),
            dma((chunks, n - 1)),
        ],
        compiler_params=pltpu.CompilerParams(
            collective_id=0, has_side_effects=True, vmem_limit_bytes=60 * 1024 * 1024
        ),
        name="conv_stack",
    )(
        stream,
        docs,
        w_value,
        w_gate,
        conv_kernel,
        conv_gain,
        conv_shift,
        w_proj,
        out_gain,
        out_shift,
    )


def solution(mesh):
    in_specs = (
        P("sp", "tp"),
        P("sp"),
        P(None, None, "tp"),
        P(None, None, "tp"),
        P(None, None, "tp"),
        P(),
        P(),
        P(None, None, "tp"),
        P(),
        P(),
    )
    return jax.shard_map(
        functools.partial(on_device, mesh.shape["tp"], mesh.shape["sp"]),
        mesh=mesh,
        in_specs=in_specs,
        out_specs=P("sp", "tp"),
        check_vma=False,
    )
```

```python
import functools

import jax
import jax.numpy as jnp
from jax import lax
from jax.experimental import pallas as pl
from jax.experimental.pallas import tpu as pltpu
from jax.sharding import PartitionSpec as P

KERNEL = 31
HALF = 15
PAD = 16
LANES = 128
ROW_BLOCK = 16
CONV_BLOCK = 32
SUM_BLOCK = 32
ALPHA = 2.0**0.25
EPS = 1e-05
MESH = pl.DeviceIdType.MESH


SIZES = (64, 96, 64, 96, 64)
DIRECT = ()
FIRST = (
    ("send", 0),
    ("send", 1),
    ("send", 2),
    ("hr1", 0),
    ("hr0", 0),
    ("hr1", 1),
    ("hr0", 1),
    ("hr1", 2),
    ("send", 3),
    ("hr0", 2),
    ("glu", 0),
    ("send", 4),
    ("docs", 0),
)
REPEAT = (
    ("glu", 1, 0),
    ("hr0", 3, 0),
    ("hr1", 3, 0),
    ("conv", 0, 0),
    ("glu", 2, 0),
    ("hr1", 4, 0),
    ("hr0", 4, 0),
    ("conv", 1, 0),
    ("glu", 3, 0),
    ("conv", 2, 0),
    ("glu", 4, 0),
    ("cr1", 1, 0),
    ("cr1", 0, 0),
    ("cr0", 1, 0),
    ("cr0", 0, 0),
    ("conv", 3, 0),
    ("conv", 4, 0),
    ("proj", 1, 0),
    ("proj", 0, 0),
    ("cr1", 2, 0),
    ("cr0", 2, 0),
    ("cr1", 3, 0),
    ("hr1", 1, 1),
    ("cr0", 3, 0),
    ("hr1", 0, 1),
    ("hr0", 0, 1),
    ("hr0", 1, 1),
    ("cr0", 4, 0),
    ("cr1", 4, 0),
    ("proj", 2, 0),
    ("proj", 3, 0),
    ("glu", 0, 1),
    ("hr1", 2, 1),
    ("hr0", 2, 1),
    ("proj", 4, 0),
)


def split(rows):
    return SIZES if sum(SIZES) == rows else (96,) * (rows // 96)


def plan(chunks):
    if chunks == len(SIZES):
        return FIRST, REPEAT
    first = [("send", p) for p in range(chunks)] + [("docs", 0)]
    repeat = [("hr%d" % i, p, 0) for p in range(chunks) for i in range(2)]
    repeat += [("glu", p, 0) for p in range(chunks)]
    repeat += [("conv", p, 0) for p in range(chunks)]
    repeat += [("cr%d" % i, p, 0) for p in range(chunks) for i in range(2)]
    repeat += [("proj", p, 0) for p in range(chunks)]
    return first, repeat


def sigmoid(v):
    return 0.5 * jnp.tanh(0.5 * v) + 0.5


def silu_of_half(u):
    return u * jnp.tanh(u) + u


def kernel(
    n,
    n_sp,
    first,
    repeat,
    stream,
    docs_hbm,
    wv_hbm,
    wg_hbm,
    taps_hbm,
    conv_gain_hbm,
    conv_shift_hbm,
    wp_hbm,
    out_gain_hbm,
    out_shift_hbm,
    out,
    docs,
    taps_in,
    conv_gain_in,
    conv_shift_in,
    out_gain_in,
    out_shift_in,
    conv_gain,
    conv_shift,
    out_gain,
    out_shift,
    wv,
    wg,
    wp,
    hbuf,
    cbuf,
    hn,
    act,
    glu,
    docpad,
    taps,
    zf,
    st_send,
    st_recv,
    means,
    scales,
    in_sem,
    w_sem,
    s_sem,
    r_sem,
    hs_sem,
    hr_sem,
    ds_sem,
    dr_sem,
    ss_sem,
    sr_sem,
):
    rows, local_d = stream.shape
    layers, width, local_c = wv.shape
    groups = local_c // LANES
    sizes = split(rows)
    chunks = len(sizes)
    ends = [sum(sizes[: p + 1]) for p in range(chunks)]
    relayed = n == 4
    me = lax.axis_index("tp")
    sp = lax.axis_index("sp")
    parity = lax.rem(sp, 2)

    def wait_weight(i, layer):
        src, dst = ((wv_hbm, wv), (wg_hbm, wg), (wp_hbm, wp))[i]
        pltpu.make_async_copy(src.at[layer], dst.at[layer], w_sem.at[i, layer]).wait()

    barrier = pltpu.get_barrier_semaphore()
    for j in range(1, n):
        pl.semaphore_signal(
            barrier, inc=1, device_id={"tp": lax.rem(me + j, n)}, device_id_type=MESH
        )

    @pl.when(sp > 0)
    def _():
        pl.semaphore_signal(barrier, inc=1, device_id={"sp": sp - 1}, device_id_type=MESH)

    @pl.when(sp < n_sp - 1)
    def _():
        pl.semaphore_signal(barrier, inc=1, device_id={"sp": sp + 1}, device_id_type=MESH)

    loads = [
        pltpu.make_async_copy(src, dst, in_sem.at[i])
        for i, (src, dst) in enumerate(
            (
                (stream, hbuf.at[0, me]),
                (docs_hbm, docs),
                (taps_hbm, taps_in),
                (conv_gain_hbm, conv_gain_in),
                (conv_shift_hbm, conv_shift_in),
                (out_gain_hbm, out_gain_in),
                (out_shift_hbm, out_shift_in),
            )
        )
    ]
    for load in loads[:2]:
        load.start()
    for layer in range(layers):
        for i, (src, dst) in enumerate(((wv_hbm, wv), (wg_hbm, wg), (wp_hbm, wp))):
            pltpu.make_async_copy(src.at[layer], dst.at[layer], w_sem.at[i, layer]).start()
    for load in loads[2:]:
        load.start()

    st_send[...] = jnp.zeros((chunks, 8, LANES), jnp.float32)
    st_recv[...] = jnp.zeros((chunks, LANES, LANES), jnp.float32)

    @pl.when(sp == 0)
    def _():
        docpad[pl.ds(0, PAD), :] = jnp.full((PAD, LANES), -1, jnp.int32)
        glu[:, :, pl.ds(0, PAD), :] = jnp.zeros((layers, groups, PAD, LANES), jnp.float32)

    @pl.when(sp == n_sp - 1)
    def _():
        docpad[pl.ds(PAD + rows, PAD), :] = jnp.full((PAD, LANES), -1, jnp.int32)
        glu[:, :, pl.ds(PAD + rows, PAD), :] = jnp.zeros(
            (layers, groups, PAD, LANES), jnp.float32
        )

    beside = (sp > 0).astype(jnp.int32) + (sp < n_sp - 1).astype(jnp.int32)
    pl.semaphore_wait(barrier, n - 1 + beside)
    loads[0].wait()

    def first_row(p):
        return pl.multiple_of(ends[p] - sizes[p] + parity * (rows + sizes[p] - 2 * ends[p]), 32)

    starts = [first_row(p) for p in range(chunks)]

    if relayed:
        near_x = me + 1 - 2 * lax.rem(me, 2)
        near_y = me + 2 - 4 * (me // 2)

    def own_copies(buf, layer, kind, p):
        a = 2 * layer + kind
        half = sizes[p] // 2
        if relayed:
            plan = [(near_x, 0, 0), (near_y, half, 1), (near_x, half, 4), (near_y, 0, 5)]
            size = half
        else:
            plan = [(lax.rem(me + j, n), 0, j - 1) for j in range(1, n)]
            size = sizes[p]
        copies = []
        for peer, offset, i in plan:
            part = pl.ds(pl.multiple_of(starts[p] + offset, 16), size)
            block = buf.at[layer, me, part, :]
            copies.append(
                pltpu.make_async_remote_copy(
                    src_ref=block,
                    dst_ref=block,
                    send_sem=s_sem.at[a, p, i],
                    recv_sem=r_sem.at[a, p, i],
                    device_id={"tp": peer},
                    device_id_type=MESH,
                )
            )
        return copies

    def relay_copies(buf, layer, kind, p):
        a = 2 * layer + kind
        half = sizes[p] // 2
        out_copies = []
        for i, (origin, target) in enumerate(((near_x, near_y), (near_y, near_x))):
            part = buf.at[
                layer, origin, pl.ds(pl.multiple_of(starts[p] + i * half, 16), half), :
            ]
            out_copies.append(
                pltpu.make_async_remote_copy(
                    src_ref=part,
                    dst_ref=part,
                    send_sem=s_sem.at[a, p, 2 + i],
                    recv_sem=r_sem.at[a, p, 2 + i],
                    device_id={"tp": target},
                    device_id_type=MESH,
                )
            )
        return out_copies

    def send(buf, layer, kind, p):
        for copy in own_copies(buf, layer, kind, p):
            copy.start()
        maybe, when = routed(layer, kind, p)
        if maybe:

            @pl.when(when)
            def _():
                for copy in far_copies(buf, layer, kind, p):
                    copy.start()

    def routed(layer, kind, p):
        return relayed and (kind, p) in DIRECT, layer == layers - 1

    def far_copies(buf, layer, kind, p):
        a = 2 * layer + kind
        half = sizes[p] // 2
        copies = []
        for i in range(2):
            part = buf.at[
                layer, me, pl.ds(pl.multiple_of(starts[p] + i * half, 16), half), :
            ]
            copies.append(
                pltpu.make_async_remote_copy(
                    src_ref=part,
                    dst_ref=part,
                    send_sem=s_sem.at[a, p, 2 + i],
                    recv_sem=r_sem.at[a, p, 2 + i],
                    device_id={"tp": 3 - me},
                    device_id_type=MESH,
                )
            )
        return copies

    def relay(buf, layer, kind, p, i):
        if relayed:
            own_copies(buf, layer, kind, p)[i].wait_recv()
            maybe, when = routed(layer, kind, p)
            if maybe:

                @pl.when(jnp.logical_not(when))
                def _():
                    relay_copies(buf, layer, kind, p)[i].start()
            else:
                relay_copies(buf, layer, kind, p)[i].start()

    def finish(buf, layer, kind, p):
        if relayed:
            for copy in own_copies(buf, layer, kind, p)[2:] + relay_copies(buf, layer, kind, p):
                copy.wait_recv()
        else:
            for copy in own_copies(buf, layer, kind, p):
                copy.wait_recv()

    def drain(buf, layer, kind, p):
        for copy in own_copies(buf, layer, kind, p):
            copy.wait_send()
        if relayed:
            for copy in relay_copies(buf, layer, kind, p):
                copy.wait_send()

    def edge(e):
        side = lax.rem(parity + e, 2)
        partner = sp - 1 + 2 * side
        there = (partner >= 0) & (partner < n_sp)
        src = pl.multiple_of(PAD + side * (rows - PAD), PAD)
        dst = pl.multiple_of((1 - side) * (PAD + rows), PAD)
        return partner, there, src, dst

    def halo_copy(layer, e):
        partner, there, src, dst = edge(e)
        return there, pltpu.make_async_remote_copy(
            src_ref=glu.at[layer, :, pl.ds(src, PAD), :],
            dst_ref=glu.at[layer, :, pl.ds(dst, PAD), :],
            send_sem=hs_sem.at[layer, e],
            recv_sem=hr_sem.at[layer, e],
            device_id={"sp": partner},
            device_id_type=MESH,
        )

    def doc_copy(e):
        partner, there, src, dst = edge(e)
        return there, pltpu.make_async_remote_copy(
            src_ref=docpad.at[pl.ds(src, PAD), :],
            dst_ref=docpad.at[pl.ds(dst, PAD), :],
            send_sem=ds_sem.at[e],
            recv_sem=dr_sem.at[e],
            device_id={"sp": partner},
            device_id_type=MESH,
        )

    def on(pair, what):
        there, copy = pair

        @pl.when(there)
        def _():
            getattr(copy, what)()

    def normalize(size, load, store, gain, shift, piece, finish_with):
        lanes = range(piece // LANES)

        count = width // LANES

        def measure(i, carry):
            at = pl.multiple_of(i * SUM_BLOCK, SUM_BLOCK)
            pivot = None
            for s in range(n):
                part = load(s, at, SUM_BLOCK)
                for g in lanes:
                    value = part[:, g * LANES : (g + 1) * LANES].astype(jnp.float32)
                    if pivot is None:
                        pivot = value
                        first = jnp.zeros_like(value)
                        second = jnp.zeros_like(value)
                    else:
                        off = value - pivot
                        first = first + off
                        second = second + off * off
            middle = first * (1.0 / count)
            means[pl.ds(at, SUM_BLOCK), :] = pivot + middle
            scales[pl.ds(at, SUM_BLOCK), :] = jnp.maximum(second - first * middle, 0.0)
            return carry

        lax.fori_loop(0, size // SUM_BLOCK, measure, 0, unroll=True)
        every = pl.ds(0, size)
        middle = means[every, :]
        mean = jnp.sum(middle, axis=1, keepdims=True) * (1.0 / LANES)
        off = middle - mean
        spread = jnp.sum(scales[every, :] + off * off * count, axis=1, keepdims=True)
        means[every, :] = jnp.broadcast_to(mean, (size, LANES))
        scales[every, :] = jnp.broadcast_to(
            lax.rsqrt(spread * (1.0 / width) + EPS), (size, LANES)
        )

        def body(i, carry):
            at = pl.multiple_of(i * ROW_BLOCK, ROW_BLOCK)
            mean = means[pl.ds(at, ROW_BLOCK), :]
            scale = scales[pl.ds(at, ROW_BLOCK), :]
            for s in range(n):
                part = load(s, at, ROW_BLOCK)
                for g in lanes:
                    value = part[:, g * LANES : (g + 1) * LANES].astype(jnp.float32)
                    column = s * piece + g * LANES
                    value = (value - mean) * scale * gain(column) + shift(column)
                    store(s, at, g * LANES, finish_with(value).astype(jnp.bfloat16))
            return carry

        lax.fori_loop(0, size // ROW_BLOCK, body, 0, unroll=True)

    def make_glu(layer, p):
        r0 = starts[p]
        size = sizes[p]
        span = pl.ds(r0, size)

        @pl.when(layer == 0)
        def _():
            for s in range(n):
                hn[span, pl.ds(s * local_d, local_d)] = hbuf[0, s, span, :]

        @pl.when(layer > 0)
        def _():
            before = jnp.maximum(layer - 1, 0)
            normalize(
                size,
                lambda s, at, count: hbuf[layer, s, pl.ds(r0 + at, count), :],
                lambda s, at, c, v: hn.__setitem__(
                    (pl.ds(r0 + at, ROW_BLOCK), pl.ds(s * local_d + c, LANES)), v
                ),
                lambda c: out_gain[before, :, pl.ds(c, LANES)],
                lambda c: out_shift[before, :, pl.ds(c, LANES)],
                local_d,
                lambda v: v,
            )

        x = hn[span, :]
        lin = jnp.dot(x, wv[layer], preferred_element_type=jnp.float32)
        gat = jnp.dot(x, wg[layer], preferred_element_type=jnp.float32)
        gated = (lin * sigmoid(gat)).astype(jnp.bfloat16).astype(jnp.float32)
        at = pl.multiple_of(r0 + PAD, PAD)
        for g in range(groups):
            glu[layer, g, pl.ds(at, size), :] = gated[:, g * LANES : (g + 1) * LANES]

    def convolve(layer, p):
        r0 = starts[p]

        def body(i, carry):
            t0 = pl.multiple_of(r0 + i * CONV_BLOCK, CONV_BLOCK)
            centre = docpad[pl.ds(t0 + PAD, CONV_BLOCK), :]
            totals = [jnp.zeros((CONV_BLOCK, LANES), jnp.float32) for _ in range(groups)]
            for k in range(KERNEL):
                at = pl.ds(t0 + k + PAD - HALF, CONV_BLOCK)
                keep = docpad[at, :] == centre
                for g in range(groups):
                    tap = taps[layer, pl.ds(k, 1), pl.ds(g * LANES, LANES)]
                    totals[g] = totals[g] + jnp.where(keep, glu[layer, g, at, :], 0.0) * tap
            for g in range(groups):
                cbuf[layer, me, pl.ds(t0, CONV_BLOCK), pl.ds(g * LANES, LANES)] = totals[
                    g
                ].astype(jnp.bfloat16)
            return carry

        lax.fori_loop(0, sizes[p] // CONV_BLOCK, body, 0, unroll=True)

    def project(layer, p):
        r0 = starts[p]
        size = sizes[p]
        span = pl.ds(r0, size)
        normalize(
            size,
            lambda s, at, count: cbuf[layer, s, pl.ds(r0 + at, count), :],
            lambda s, at, c, v: act.__setitem__(
                (pl.ds(at, ROW_BLOCK), pl.ds(s * local_c + c, LANES)), v
            ),
            lambda c: conv_gain[layer, :, pl.ds(c, LANES)],
            lambda c: conv_shift[layer, :, pl.ds(c, LANES)],
            local_c,
            silu_of_half,
        )
        z = jnp.dot(act[pl.ds(0, size), :], wp[layer], preferred_element_type=jnp.float32)
        own = hn[span, pl.ds(pl.multiple_of(me * local_d, LANES), local_d)]
        z = z + ALPHA * own.astype(jnp.float32)

        @pl.when(layer < layers - 1)
        def _():
            after = jnp.minimum(layer + 1, layers - 1)
            hbuf[after, me, span, :] = z.astype(jnp.bfloat16)
            send(hbuf, after, 0, p)

        @pl.when(layer == layers - 1)
        def _():
            zf[span, :] = z
            total = jnp.sum(z, axis=1, keepdims=True)
            off = z - total * (1.0 / local_d)
            spread = jnp.sum(off * off, axis=1, keepdims=True)
            lane = lax.broadcasted_iota(jnp.int32, (size, LANES), 1)
            tile = jnp.where(lane == 0, total, jnp.where(lane == 1, spread, 0.0))
            stats = jnp.transpose(tile)[:8, :]
            st_send[p, :, pl.ds(0, size)] = stats
            st_recv[p, pl.ds(pl.multiple_of(me * 8, 8), 8), pl.ds(0, size)] = stats
            for copy in stat_copies(p):
                copy.start()

    def stat_copies(p):
        return [
            pltpu.make_async_remote_copy(
                src_ref=st_send.at[p],
                dst_ref=st_recv.at[p, pl.ds(pl.multiple_of(me * 8, 8), 8), :],
                send_sem=ss_sem.at[p, j - 1],
                recv_sem=sr_sem.at[p, j - 1],
                device_id={"tp": lax.rem(me + j, n)},
                device_id_type=MESH,
            )
            for j in range(1, n)
        ]

    lead = [p for what, p, _ in repeat if what == "proj"][0]

    def prepare():
        loads[1].wait()
        for i in range(rows // LANES):
            row = jnp.broadcast_to(docs[pl.ds(i, 1), :], (LANES, LANES))
            docpad[pl.ds(PAD + i * LANES, LANES), :] = jnp.transpose(row)
        for e in range(2):
            on(doc_copy(e), "start")
        for load in loads[2:]:
            load.wait()
        taps[:, pl.ds(0, KERNEL), :] = taps_in[...].astype(jnp.float32)
        for layer in range(layers):
            conv_gain[layer] = 0.5 * conv_gain_in[pl.ds(layer, 1), :]
            conv_shift[layer] = 0.5 * conv_shift_in[pl.ds(layer, 1), :]
            out_gain[layer] = out_gain_in[pl.ds(layer, 1), :]
            out_shift[layer] = out_shift_in[pl.ds(layer, 1), :]

    def step(what, p, layer):
        if what == "send":
            send(hbuf, 0, 0, p)
        elif what in ("hr0", "hr1"):
            relay(hbuf, layer, 0, p, int(what[2]))
        elif what in ("cr0", "cr1"):
            relay(cbuf, layer, 1, p, int(what[2]))
        elif what == "glu":
            finish(hbuf, layer, 0, p)
            if p == 0:
                wait_weight(0, layer)
                wait_weight(1, layer)
            make_glu(layer, p)
            if p == 0:
                on(halo_copy(layer, 0), "start")
            if p == chunks - 1:
                on(halo_copy(layer, 1), "start")
        elif what == "conv":
            if p == 0:
                on(halo_copy(layer, 0), "wait_recv")
            if p == chunks - 1:
                on(halo_copy(layer, 1), "wait_recv")
            convolve(layer, p)
            send(cbuf, layer, 1, p)
        elif what == "proj":
            if p == lead:
                wait_weight(2, layer)
            finish(cbuf, layer, 1, p)
            project(layer, p)

    for what, p in first:
        if what == "docs":
            prepare()
        else:
            step(what, p, 0)

    def one_layer(layer, carry):
        for what, p, ahead in repeat:
            if ahead:

                @pl.when(layer < layers - 1)
                def _():
                    step(what, p, jnp.minimum(layer + 1, layers - 1))
            else:
                step(what, p, layer)
        return carry

    for e in range(2):
        on(doc_copy(e), "wait_recv")
    lax.fori_loop(0, layers, one_layer, 0)

    at_d = pl.ds(pl.multiple_of(me * local_d, LANES), local_d)
    gain = out_gain[layers - 1, :, at_d]
    shift = out_shift[layers - 1, :, at_d]
    for p in range(chunks):
        for copy in stat_copies(p):
            copy.wait_recv()
        stats = jnp.transpose(st_recv[p])[: sizes[p]]
        total = stats[:, 0:1]
        for s in range(1, n):
            total = total + stats[:, 8 * s : 8 * s + 1]
        mean = total * (1.0 / width)
        spread = jnp.zeros_like(mean)
        for s in range(n):
            off = stats[:, 8 * s : 8 * s + 1] * (1.0 / local_d) - mean
            spread = spread + stats[:, 8 * s + 1 : 8 * s + 2] + off * off * local_d
        scale = lax.rsqrt(spread * (1.0 / width) + EPS)
        span = pl.ds(starts[p], sizes[p])
        out[span, :] = ((zf[span, :] - mean) * scale * gain + shift).astype(jnp.bfloat16)

    def drain_layer(layer, carry):
        for p in range(chunks):
            drain(hbuf, layer, 0, p)
            drain(cbuf, layer, 1, p)
        for e in range(2):
            on(halo_copy(layer, e), "wait_send")
        return carry

    lax.fori_loop(0, layers, drain_layer, 0)
    for e in range(2):
        on(doc_copy(e), "wait_send")
    for p in range(chunks):
        for copy in stat_copies(p):
            copy.wait_send()


def on_device(
    n,
    n_sp,
    stream,
    doc_ids,
    w_value,
    w_gate,
    conv_kernel,
    conv_gain,
    conv_shift,
    w_proj,
    out_gain,
    out_shift,
):
    rows, local_d = stream.shape
    layers, width, local_c = w_value.shape
    sizes = split(rows)
    chunks, tall = len(sizes), max(sizes)
    first, repeat = plan(chunks)
    docs = doc_ids.reshape(rows // LANES, LANES)
    vmem = pl.BlockSpec(memory_space=pltpu.VMEM)
    hbm = pl.BlockSpec(memory_space=pl.ANY)
    ways = 6 if n == 4 else n - 1
    dma = pltpu.SemaphoreType.DMA
    return pl.pallas_call(
        functools.partial(kernel, n, n_sp, first, repeat),
        out_shape=pltpu.VMEM((rows, local_d), jnp.bfloat16),
        in_specs=[hbm] * 10,
        out_specs=vmem,
        scratch_shapes=[
            pltpu.VMEM(docs.shape, jnp.int32),
            pltpu.VMEM(conv_kernel.shape, jnp.bfloat16),
            pltpu.VMEM((layers, width), jnp.float32),
            pltpu.VMEM((layers, width), jnp.float32),
            pltpu.VMEM((layers, width), jnp.float32),
            pltpu.VMEM((layers, width), jnp.float32),
            pltpu.VMEM((layers, 1, width), jnp.float32),
            pltpu.VMEM((layers, 1, width), jnp.float32),
            pltpu.VMEM((layers, 1, width), jnp.float32),
            pltpu.VMEM((layers, 1, width), jnp.float32),
            pltpu.VMEM((layers, width, local_c), jnp.bfloat16),
            pltpu.VMEM((layers, width, local_c), jnp.bfloat16),
            pltpu.VMEM((layers, local_c * n, local_d), jnp.bfloat16),
            pltpu.VMEM((layers, n, rows, local_d), jnp.bfloat16),
            pltpu.VMEM((layers, n, rows, local_c), jnp.bfloat16),
            pltpu.VMEM((rows, n * local_d), jnp.bfloat16),
            pltpu.VMEM((tall, n * local_c), jnp.bfloat16),
            pltpu.VMEM((layers, local_c // LANES, rows + 2 * PAD, LANES), jnp.float32),
            pltpu.VMEM((rows + 2 * PAD, LANES), jnp.int32),
            pltpu.VMEM((layers, 32, local_c), jnp.float32),
            pltpu.VMEM((rows, local_d), jnp.float32),
            pltpu.VMEM((chunks, 8, LANES), jnp.float32),
            pltpu.VMEM((chunks, LANES, LANES), jnp.float32),
            pltpu.VMEM((tall, LANES), jnp.float32),
            pltpu.VMEM((tall, LANES), jnp.float32),
            dma((7,)),
            dma((3, layers)),
            dma((2 * layers, chunks, ways)),
            dma((2 * layers, chunks, ways)),
            dma((layers, 2)),
            dma((layers, 2)),
            dma((2,)),
            dma((2,)),
            dma((chunks, n - 1)),
            dma((chunks, n - 1)),
        ],
        compiler_params=pltpu.CompilerParams(
            collective_id=0, has_side_effects=True, vmem_limit_bytes=60 * 1024 * 1024
        ),
        name="conv_stack",
    )(
        stream,
        docs,
        w_value,
        w_gate,
        conv_kernel,
        conv_gain,
        conv_shift,
        w_proj,
        out_gain,
        out_shift,
    )


def solution(mesh):
    in_specs = (
        P("sp", "tp"),
        P("sp"),
        P(None, None, "tp"),
        P(None, None, "tp"),
        P(None, None, "tp"),
        P(),
        P(),
        P(None, None, "tp"),
        P(),
        P(),
    )
    return jax.shard_map(
        functools.partial(on_device, mesh.shape["tp"], mesh.shape["sp"]),
        mesh=mesh,
        in_specs=in_specs,
        out_specs=P("sp", "tp"),
        check_vma=False,
    )
```
